512 devices in a mesh: sp: 64 (over z, y), tp: 8 (over x, core).
Axes of the slice: x: 4, y: 8, z: 8, core: 2. Of those that a mesh axis runs over, the one named last changes fastest.
Arguments:
- queries: bfloat16 [16384, 1024], P('sp', 'tp'), may hold values from -6 to 6
- keys: bfloat16 [16384, 256], P('sp'), may hold values from -6 to 6
- values: bfloat16 [16384, 256], P('sp'), may hold values from -6 to 6
- query_gain: float32 [128], replicated, may hold values from 1.4 to 5.5
- key_gain: float32 [128], replicated, may hold values from 1.4 to 5.5
- residual_in: bfloat16 [16384, 2048], P(('sp', 'tp')), may hold values from -6 to 6
- out_weight: bfloat16 [1024, 2048], P('tp'), may hold values from -0.1875 to 0.1875
- norm_gain: float32 [2048], replicated, may hold values from 0.1 to 1.9
- gate_weight: bfloat16 [2048, 3072], P('sp', 'tp'), may hold values from -0.125 to 0.125
- up_weight: bfloat16 [2048, 3072], P('sp', 'tp'), may hold values from -0.125 to 0.125
- down_weight: bfloat16 [3072, 2048], P('tp', 'sp'), may hold values from -0.109375 to 0.109375
Outputs:
- result: bfloat16 [16384, 2048], P(('sp', 'tp'))
The draws below stay inside these ranges and needn't reach their ends.
All inputs are finite; a program needn't handle non-finite values.
Results may differ from the reference program's by a relative error of at most 0.017.
Values may be sent and summed in bfloat16 or wider, within the bound.
A program may use at most 64 MiB of HBM per device.

```python
import math
import jax
import jax.numpy as jnp
from jax import lax

D = 2048
FF = 3072
HEAD = 128
Q_HEADS = 8
KV_HEADS = 2
GRID_WIDTH = 64
TOKENS = 16384
N_TP = 8


def raw_keys(key):
    drawn = jax.random.normal(jax.random.fold_in(key, 11), (TOKENS, KV_HEADS * HEAD), jnp.float32)
    return jnp.clip(drawn, -6.0, 6.0)


def draw_keys(key, part):
    return raw_keys(key).astype(jnp.bfloat16)


def draw_queries(key, part):
    background = jnp.clip(jax.random.normal(jax.random.fold_in(key, 12), (TOKENS, Q_HEADS * HEAD), jnp.float32), -6.0, 6.0)
    return background.astype(jnp.bfloat16)


def draw_values(key, part):
    offset = 1.5 * jax.random.normal(jax.random.fold_in(key, 31), (1, KV_HEADS * HEAD), jnp.float32)
    noise = jax.random.normal(jax.random.fold_in(key, 32), (TOKENS, KV_HEADS * HEAD), jnp.float32)
    return jnp.clip(offset + noise, -6.0, 6.0).astype(jnp.bfloat16)


def draw_gain(key, salt):
    return jax.random.uniform(jax.random.fold_in(key, salt), (HEAD,), jnp.float32, 1.4, 2.0)


def draw_query_gain(key, part):
    return draw_gain(key, 21)


def draw_key_gain(key, part):
    return draw_gain(key, 22)


def levels(stream_key, extent, cuts, smallest, high):
    factor_of, own = 1.0, jax.random.fold_in(stream_key, 6)
    for axis_at, parts in cuts:
        draws = jnp.exp(jax.random.uniform(jax.random.fold_in(own, axis_at), (parts,), jnp.float32, smallest / len(cuts), high / len(cuts)))
        factor_of = factor_of * jnp.repeat(draws, extent[axis_at] // parts).reshape([-1 if axis == axis_at else 1 for axis in range(len(extent))])
    return factor_of


def centred(own_key, extent, scale, most, cuts=(), kind=jnp.bfloat16):
    loudness = levels(own_key, extent, cuts, -0.22, 0.18) if cuts else 1.0
    entries = jax.random.normal(own_key, extent, jnp.float32) * scale * loudness
    return jnp.minimum(jnp.maximum(entries, -most), most).astype(kind)


def setup_inputs(seed: int = 0) -> dict:
    seeds = jax.random.split(jax.random.key(seed), 12)
    queries = draw_queries(jax.random.fold_in(seeds[11], 71), 0)
    keys = draw_keys(jax.random.fold_in(seeds[11], 71), 0)
    values = draw_values(jax.random.fold_in(seeds[11], 71), 0)
    query_gain = draw_query_gain(jax.random.fold_in(seeds[11], 71), 0)
    key_gain = draw_key_gain(jax.random.fold_in(seeds[11], 71), 0)
    residual_in = centred(seeds[5], (TOKENS, D), 1.0, 6.0, ((0, 512),))
    out_weight = centred(seeds[6], (Q_HEADS * HEAD, D), (Q_HEADS * HEAD) ** -0.5, 0.1875, ((0, 8),))
    norm_gain = jnp.clip(1.0 + 0.18 * jax.random.normal(seeds[7], (D,), jnp.float32), 0.1, 1.9)
    gate_weight = centred(seeds[8], (D, FF), D ** -0.5, 0.125, ((0, 64), (1, 8)))
    up_weight = centred(seeds[9], (D, FF), D ** -0.5, 0.125, ((0, 64), (1, 8)))
    down_weight = centred(seeds[10], (FF, D), FF ** -0.5, 0.109375, ((0, 8), (1, 64)))
    return {"queries": queries, "keys": keys, "values": values, "query_gain": query_gain, "key_gain": key_gain, "residual_in": residual_in, "out_weight": out_weight, "norm_gain": norm_gain, "gate_weight": gate_weight, "up_weight": up_weight, "down_weight": down_weight}


EPS = 1e-06
ROPE_BASE = 10000.0

def normalize(wide_values, gain):
    wide = wide_values.astype(jnp.float32)
    return wide * lax.rsqrt(lax.optimization_barrier(jnp.mean(wide * wide, axis=-1, keepdims=True)) + EPS) * gain.astype(jnp.float32)

def rotate_pair(segment, angles):
    half_size = segment.shape[-1] // 2
    first = segment[..., :half_size]
    second = segment[..., half_size:]
    cosine = jnp.cos(angles)[:, None, :]
    sine_part = jnp.sin(angles)[:, None, :]
    return jnp.concatenate([first * cosine - second * sine_part, second * cosine + first * sine_part], axis=-1)

def grid_rotary(head_rows, positions):
    head_size = head_rows.shape[-1]
    half_size = head_size // 2
    quarter = head_size // 4
    inverse = ROPE_BASE ** (-jnp.arange(quarter, dtype=jnp.float32) * 2.0 / half_size)
    row_angles = (positions // GRID_WIDTH).astype(jnp.float32)[:, None] * inverse
    col_angles = (positions % GRID_WIDTH).astype(jnp.float32)[:, None] * inverse
    return jnp.concatenate([rotate_pair(head_rows[..., :half_size], row_angles), rotate_pair(head_rows[..., half_size:], col_angles)], axis=-1)

def blockwise_sum(left, right, pieces):
    width = left.shape[1] // pieces

    def add_piece(total, index):
        start = (index * width).astype(jnp.int32)
        columns = lax.dynamic_slice_in_dim(left, start, width, 1)
        rows = lax.dynamic_slice_in_dim(right, start, width, 0)
        part = jnp.dot(columns, rows, preferred_element_type=jnp.float32)
        rounded = lax.optimization_barrier(part.astype(jnp.bfloat16)).astype(jnp.float32)
        return (total + rounded, None)
    start_total = jnp.zeros((left.shape[0], right.shape[1]), jnp.float32)
    total, unused = lax.scan(add_piece, start_total, jnp.arange(pieces, dtype=jnp.int32))
    return total

def reference(queries, keys, values, query_gain, key_gain, residual_in, out_weight, norm_gain, gate_weight, up_weight, down_weight):
    token_count = queries.shape[0]
    positions = jnp.arange(token_count, dtype=jnp.int32)
    group_size = Q_HEADS // KV_HEADS
    turned_queries = grid_rotary(normalize(queries.reshape(token_count, Q_HEADS, HEAD), query_gain), positions).astype(jnp.bfloat16)
    turned_keys = grid_rotary(normalize(keys.reshape(token_count, KV_HEADS, HEAD), key_gain), positions).astype(jnp.bfloat16)
    keys_wide = turned_keys.astype(jnp.float32)
    values_wide = values.reshape(token_count, KV_HEADS, HEAD).astype(jnp.float32)
    block_rows = math.gcd(token_count, 256)
    score_scale = HEAD ** (-0.5)

    def one_block(query_block):
        grouped = query_block.astype(jnp.float32).reshape(block_rows, KV_HEADS, group_size, HEAD)
        scores = jnp.einsum('bkgd,skd->kgbs', grouped, keys_wide) * score_scale
        peak_score = lax.optimization_barrier(jnp.max(scores, axis=-1, keepdims=True))
        raw = jnp.exp(scores - peak_score)
        weight_total = lax.optimization_barrier(jnp.sum(raw, axis=-1))
        rounded = lax.optimization_barrier(raw.astype(jnp.bfloat16)).astype(jnp.float32)
        summed = jnp.einsum('kgbs,skd->bkgd', rounded, values_wide)
        scaled = summed / jnp.transpose(weight_total, (2, 0, 1))[..., None]
        return scaled.reshape(block_rows, Q_HEADS * HEAD).astype(jnp.bfloat16)
    blocked = turned_queries.reshape(token_count // block_rows, block_rows, Q_HEADS, HEAD)
    attended = lax.map(one_block, blocked).reshape(token_count, Q_HEADS * HEAD)
    attention_out = blockwise_sum(attended, out_weight, N_TP)
    middle = (residual_in.astype(jnp.float32) + attention_out).astype(jnp.bfloat16)
    normed = normalize(middle, norm_gain).astype(jnp.bfloat16)
    gate_part = jnp.dot(normed, gate_weight, preferred_element_type=jnp.float32)
    lifted = jnp.dot(normed, up_weight, preferred_element_type=jnp.float32)
    hidden = (jax.nn.silu(gate_part) * lifted).astype(jnp.bfloat16)
    mixer_out = blockwise_sum(hidden, down_weight, N_TP)
    return (middle.astype(jnp.float32) + mixer_out).astype(jnp.bfloat16)
```

```python
import math

import jax
import jax.numpy as jnp
import numpy as np
from jax import lax
from jax.experimental import pallas as pl
from jax.experimental.pallas import tpu as pltpu
from jax.sharding import Mesh
from jax.sharding import PartitionSpec as P

NZ = 8
NY = 8
RING = 8
NX = 4
HEAD = 128
GRID_WIDTH = 64
TOK = 256
TEAM = 4
KTOK = TOK // TEAM
KH = KTOK // 2
ROWS = 32
D = 2048
FFD = 384
EPS = 1e-06
ROPE_BASE = 10000.0
SCALE = HEAD ** (-0.5) * math.log2(math.e)
F32 = jnp.float32
BF16 = jnp.bfloat16
NT = (((1,), (1,)), ((), ()))


def rope_tables():
    quarter = HEAD // 4
    inverse = ROPE_BASE ** (-np.arange(quarter, dtype=np.float64) * 2.0 / (HEAD // 2))
    rows = np.arange(NZ * NY * TOK // GRID_WIDTH, dtype=np.float64)[:, None] * inverse
    cols = np.arange(GRID_WIDTH, dtype=np.float64)[:, None] * inverse

    def half(angles):
        return (
            np.concatenate([np.cos(angles), np.cos(angles)], axis=1),
            np.concatenate([-np.sin(angles), np.sin(angles)], axis=1),
        )

    rc, rs = half(rows)
    cc, cs = half(cols)
    left = lambda a: np.concatenate([a, np.zeros_like(a)], axis=1).astype(np.float32)
    right = lambda a: np.concatenate([np.zeros_like(a), a], axis=1).astype(np.float32)
    return left(rc), left(rs), right(cc), right(cs)


def normalize(x, gain):
    return x * lax.rsqrt(jnp.mean(x * x, axis=-1, keepdims=True) + EPS) * gain


def turn(x, cosine, sine):
    lane = lax.broadcasted_iota(jnp.int32, x.shape, 1)
    ahead = pltpu.roll(x, HEAD - 32, 1)
    behind = pltpu.roll(x, 32, 1)
    partner = jnp.where((lane // 32) % 2 == 0, ahead, behind)
    return x * cosine + partner * sine


def layer_kernel(
    q_ref, k_ref, v_ref, qg_ref, kg_ref, res_ref, ow_hbm, ng_ref, gate_ref, up_ref, down_ref,
    rc_ref, rs_ref, cc_ref, cs_ref,
    out_ref,
    qbuf, kv0, kv1, w, wp, ow, acc, peak, osend, orecv, att, nbuf, mid, psend, pown, precv,
    q_s, q_r, ka_s, ka_r, wa_s, wa_r, kb_s, kb_r, wb_s, wb_r, wr_s, wr_r,
    ow_l, ow_s, ow_r, o_s, o_r, n_s, n_r, p_s, p_r,
):
    z = lax.axis_index("z")
    y = lax.axis_index("y")
    x = lax.axis_index("x")
    c = lax.axis_index("c")
    tp = x * 2 + c
    team = x // 2
    j = lax.rem(x, 2) * 2 + c
    s = z * NY + y
    pos = (z, y)
    axis = ("z", "y")

    def wrap(v, n=RING):
        return lax.rem(v + n, n)

    def tp_id(i):
        return {"x": i // 2, "c": lax.rem(i, 2)}

    own_ow = pltpu.make_async_copy(ow_hbm, ow.at[tp], ow_l)
    own_ow.start()

    barrier = pltpu.get_barrier_semaphore()

    def greet(d, carry):
        pl.semaphore_signal(barrier, inc=1, device_id={"z": wrap(z + d)})
        pl.semaphore_signal(barrier, inc=1, device_id={"y": wrap(y + d)})
        pl.semaphore_signal(barrier, inc=1, device_id=tp_id(wrap(tp + d)))
        return carry

    lax.fori_loop(1, RING, greet, 0)

    k_rows = k_ref[pl.ds(pl.multiple_of(j * KTOK, KTOK), KTOK), :].astype(F32)
    v_rows = v_ref[pl.ds(pl.multiple_of(j * KTOK, KTOK), KTOK), :].astype(F32)
    kk = jnp.where(team == 0, k_rows[:, :HEAD], k_rows[:, HEAD:])
    vv = jnp.where(team == 0, v_rows[:, :HEAD], v_rows[:, HEAD:]).astype(BF16)
    cosine = rc_ref[pl.ds(s * 4 + j, 1), :] + cc_ref[...]
    sine = rs_ref[pl.ds(s * 4 + j, 1), :] + cs_ref[...]
    kk = turn(normalize(kk, kg_ref[...]), cosine, sine).astype(BF16)
    kv0[z, 0, y] = kk[:KH]
    kv0[z, 1, y] = vv[:KH]
    kv1[y, 0, z] = kk[KH:]
    kv1[y, 1, z] = vv[KH:]
    for r in range(4):
        part = slice(r * GRID_WIDTH, (r + 1) * GRID_WIDTH)
        cosine = rc_ref[pl.ds(s * 4 + r, 1), :] + cc_ref[...]
        sine = rs_ref[pl.ds(s * 4 + r, 1), :] + cs_ref[...]
        qq = turn(normalize(q_ref[part, :].astype(F32), qg_ref[...]), cosine, sine)
        qbuf[j, part] = (qq * SCALE).astype(BF16)
    w[0, z, y] = gate_ref[...].reshape(2, 16, FFD)
    w[1, z, y] = up_ref[...].reshape(2, 16, FFD)
    row = lax.broadcasted_iota(jnp.int32, (32, 32), 0)
    col = lax.broadcasted_iota(jnp.int32, (32, 32), 1)
    eye = jnp.where(row == col, 1.0, 0.0).astype(BF16)
    down_t = lax.dot_general(eye, down_ref[...], NT, preferred_element_type=F32)
    w[2, z, y] = down_t.astype(BF16).reshape(2, 16, FFD)
    peak[...] = jnp.full(peak.shape, -1e30, F32)
    acc[...] = jnp.zeros(acc.shape, F32)

    pl.semaphore_wait(barrier, 21)

    def remote(ref, dst, ss, rs, dev):
        return pltpu.make_async_remote_copy(
            src_ref=ref, dst_ref=dst, send_sem=ss, recv_sem=rs,
            device_id=dev, device_id_type=pl.DeviceIdType.MESH,
        )

    def kva(h, d):
        ref = kv0.at[z, :, y] if h == 0 else kv1.at[y, :, z]
        dev = {"y": wrap(y + d)} if h == 0 else {"z": wrap(z + d)}
        return remote(ref, ref, ka_s.at[h, d - 1], ka_r.at[h, d - 1], dev)

    def kva_in(h, d):
        ref = kv0.at[z, :, wrap(y - d)] if h == 0 else kv1.at[y, :, wrap(z - d)]
        return remote(ref, ref, ka_s.at[h, d - 1], ka_r.at[h, d - 1], {"y": y})

    def wa(h, d):
        ref = w.at[:, z, y, h]
        dev = {"y": wrap(y + d)} if h == 0 else {"z": wrap(z + d)}
        return remote(ref, ref, wa_s.at[h, d - 1], wa_r.at[h, d - 1], dev)

    def wa_in(h, d):
        ref = w.at[:, z, wrap(y - d), 0] if h == 0 else w.at[:, wrap(z - d), y, 1]
        return remote(ref, ref, wa_s.at[h, d - 1], wa_r.at[h, d - 1], {"y": y})

    def each(fn):
        def body(d, carry):
            fn(d)
            return carry

        lax.fori_loop(1, RING, body, 0)

    def start_kva(d):
        kva(0, d).start()
        kva(1, d).start()

    each(start_kva)

    def qcopy(d):
        other = team * TEAM + lax.rem(j + d, TEAM)
        return remote(qbuf.at[j], qbuf.at[j], q_s.at[d - 1], q_r.at[d - 1], tp_id(other))

    def qcopy_in(d):
        ref = qbuf.at[lax.rem(j - d + TEAM, TEAM)]
        return remote(ref, ref, q_s.at[d - 1], q_r.at[d - 1], tp_id(tp))

    for d in range(1, TEAM):
        qcopy(d).start()

    right_x = {"x": wrap(x + 1, NX)}
    left_x = {"x": wrap(x - 1, NX)}
    partner = {"c": 1 - c}
    tl = wrap(x - 1, NX) * 2 + c
    tr = wrap(x + 1, NX) * 2 + c
    far = wrap(x + 2, NX) * 2 + c

    def head_ref(i, part=None):
        if part is None:
            return ow.at[i]
        return ow.at[i, pl.ds(part * 64, 64)]

    def owcopy(n, ref, dev):
        return remote(ref, ref, ow_s.at[n], ow_r.at[n], dev)

    ow_out = [
        owcopy(0, head_ref(tp), right_x),
        owcopy(1, head_ref(tp), left_x),
        owcopy(2, head_ref(tp), partner),
        owcopy(3, head_ref(tl, 0), right_x),
        owcopy(4, head_ref(tr, 1), left_x),
        owcopy(5, head_ref(tl), partner),
        owcopy(6, head_ref(tr), partner),
        owcopy(7, head_ref(far, 0), partner),
        owcopy(8, head_ref(far, 1), partner),
    ]
    flip = 1 - 2 * c
    ow_in = [
        owcopy(0, head_ref(tl), right_x),
        owcopy(1, head_ref(tr), left_x),
        owcopy(2, head_ref(tp + flip), partner),
        owcopy(3, head_ref(far, 0), right_x),
        owcopy(4, head_ref(far, 1), left_x),
        owcopy(5, head_ref(tl + flip), partner),
        owcopy(6, head_ref(tr + flip), partner),
        owcopy(7, head_ref(far + flip, 0), partner),
        owcopy(8, head_ref(far + flip, 1), partner),
    ]
    own_ow.wait()

    def start_wa(d):
        wa(0, d).start()
        wa(1, d).start()

    each(start_wa)
    for n in range(3):
        ow_out[n].start()

    def kvb(h, d, k, m, incoming):
        shift = (k if incoming else k - 1) * (-1 if d == 0 else 1)
        buf = kv0 if h == 0 else kv1
        ref = buf.at[wrap(pos[h] + shift), m]
        dev = {axis[h]: wrap(pos[h] + (1 if d == 0 else -1))}
        return remote(ref, ref, kb_s.at[h, d, k - 1, m], kb_r.at[h, d, k - 1, m], dev)

    def kv_steps(k):
        return [(h, d, m) for m in range(2) for h in range(2) for d in range(2) if k < 4 or d == m]

    def kv_send(k):
        for h, d, m in kv_steps(k):
            if k > 1:
                kvb(h, d, k - 1, m, True).wait_recv()
            kvb(h, d, k, m, False).start()
        if k == 4:
            for h, d, m in kv_steps(3):
                if d != m:
                    kvb(h, d, 3, m, True).wait_recv()

    def w_block(h, b, m, lo, hi):
        if h == 0:
            return lambda buf: buf.at[m, b, lo:hi, 0]
        return lambda buf: buf.at[m, lo:hi, b, 1]

    def wb(h, d, k, m, incoming):
        shift = (k if incoming else k - 1) * (-1 if d == 0 else 1)
        lo, hi = (0, RING) if k < 4 else ((0, 4) if d == 0 else (4, RING))
        ref = w_block(h, wrap(pos[h] + shift), m, lo, hi)(w)
        dev = {axis[h]: wrap(pos[h] + (1 if d == 0 else -1))}
        return remote(ref, ref, wb_s.at[h, d, k - 1, m], wb_r.at[h, d, k - 1, m], dev)

    def hand_over(h, d, k, m):
        shift = k * (-1 if d == 0 else 1)
        lo, hi = (0, RING) if k < 4 else ((0, 4) if d == 0 else (4, RING))
        pick = w_block(h, wrap(pos[h] + shift), m, lo, hi)
        remote(pick(w), pick(wp), wr_s.at[m], wr_r.at[m], partner).start()

    def pump(p):
        k, m = p // 3 + 1, p % 3
        for h in range(2):
            for d in range(2):
                if k > 1:
                    wb(h, d, k - 1, m, True).wait_recv()
                if k <= 4:
                    wb(h, d, k, m, False).start()
        for h in range(2):
            for d in range(2):
                if k > 1:
                    hand_over(h, d, k - 1, m)
                elif d == 0:
                    hand_over(h, 0, 0, m)

    ones = jnp.ones((1, HEAD), BF16)

    def attend(blocks):
        keys = jnp.concatenate([buf[b, 0].reshape(256, HEAD) for buf, b in blocks], axis=0)
        vals = jnp.concatenate([buf[b, 1].reshape(256, HEAD) for buf, b in blocks], axis=0)
        wide = keys.shape[0]
        vals = jnp.concatenate([vals, jnp.broadcast_to(ones, vals.shape)], axis=1)

        def one_head(h, carry):
            scores = lax.dot_general(qbuf[h], keys, NT, preferred_element_type=F32)
            old = peak[h]
            new = jnp.maximum(old, jnp.max(scores, axis=1, keepdims=True))
            factor = jnp.exp2(old - new)
            peak[h] = new
            raw = jnp.exp2(scores - jnp.concatenate([new] * (wide // HEAD), axis=1)).astype(BF16)
            update = jnp.dot(raw, vals, preferred_element_type=F32)
            acc[h] = acc[h] * jnp.concatenate([factor, factor], axis=1) + update
            return carry

        lax.fori_loop(0, TEAM, one_head, 0)

    def wait_kva(d):
        kva_in(0, d).wait_recv()
        kva_in(1, d).wait_recv()

    def wait_wa(d):
        wa_in(0, d).wait_recv()
        wa_in(1, d).wait_recv()

    each(wait_kva)
    kv_send(1)
    for d in range(1, TEAM):
        qcopy_in(d).wait_recv()
    attend([(kv0, z), (kv1, y)])
    kv_send(2)
    each(wait_wa)
    pump(0)
    attend([(kv0, wrap(z - 1)), (kv0, wrap(z + 1)), (kv1, wrap(y - 1)), (kv1, wrap(y + 1))])
    kv_send(3)
    pump(1)
    attend([(kv0, wrap(z - 2)), (kv0, wrap(z + 2)), (kv1, wrap(y - 2)), (kv1, wrap(y + 2))])
    kv_send(4)
    pump(2)
    ow_in[0].wait_recv()
    ow_out[3].start()
    ow_in[1].wait_recv()
    ow_out[4].start()
    ow_out[5].start()
    ow_out[6].start()
    attend([(kv0, wrap(z - 3)), (kv0, wrap(z + 3)), (kv1, wrap(y - 3)), (kv1, wrap(y + 3))])
    for h, d, m in kv_steps(4):
        kvb(h, d, 4, m, True).wait_recv()
    pump(3)
    attend([(kv0, wrap(z + 4)), (kv1, wrap(y + 4))])

    lane = lax.broadcasted_iota(jnp.int32, (TOK, HEAD), 1)
    stats = jnp.zeros((TOK, HEAD), F32)
    for h in range(TEAM):
        total = acc[h, :, HEAD:]
        mean = (acc[h, :, :HEAD] / total).astype(BF16)
        osend[:, :, h * HEAD : (h + 1) * HEAD] = mean.reshape(8, ROWS, HEAD)
        level = peak[h] + jnp.log2(total)
        first = level.astype(BF16).astype(F32)
        second = (level - first).astype(BF16).astype(F32)
        third = level - first - second
        stats = jnp.where(lane == h, first, stats)
        stats = jnp.where(lane == h + 4, second, stats)
        stats = jnp.where(lane == h + 8, third, stats)
    osend[:, :, TEAM * HEAD :] = stats.astype(BF16).reshape(8, ROWS, HEAD)

    def ocopy(d):
        i = wrap(tp + d)
        return remote(osend.at[i], orecv.at[tp], o_s.at[d - 1], o_r.at[d - 1], tp_id(i))

    def ocopy_in(d):
        ref = orecv.at[wrap(tp - d)]
        return remote(ref, ref, o_s.at[d - 1], o_r.at[d - 1], tp_id(tp))

    each(lambda d: ocopy(d).start())
    orecv[tp] = osend[tp]

    ow_in[3].wait_recv()
    ow_out[7].start()
    ow_in[4].wait_recv()
    ow_out[8].start()
    pump(4)
    pump(5)

    each(lambda d: ocopy_in(d).wait_recv())
    for t in range(2):
        for h in range(TEAM):
            levels = []
            for i in range(t * TEAM, (t + 1) * TEAM):
                st = orecv[i, :, TEAM * HEAD :].astype(F32)
                levels.append(st[:, h : h + 1] + st[:, h + 4 : h + 5] + st[:, h + 8 : h + 9])
            top = jnp.maximum(jnp.maximum(levels[0], levels[1]), jnp.maximum(levels[2], levels[3]))
            shares = [jnp.exp2(v - top) for v in levels]
            total = shares[0] + shares[1] + shares[2] + shares[3]
            mixed = jnp.zeros((ROWS, HEAD), F32)
            for i in range(TEAM):
                block = orecv[t * TEAM + i, :, h * HEAD : (h + 1) * HEAD].astype(F32)
                mixed = mixed + block * shares[i]
            at = (t * TEAM + h) * HEAD
            att[:, at : at + HEAD] = (mixed / total).astype(BF16)

    for n in (2, 5, 6, 7, 8):
        ow_in[n].wait_recv()
    projected = jnp.dot(att[...], ow[...].reshape(8 * HEAD, D), preferred_element_type=F32)
    middle = (res_ref[...].astype(F32) + projected).astype(BF16)
    mid[...] = middle
    nbuf[x] = normalize(middle.astype(F32), ng_ref[...]).astype(BF16)

    def ncopy(n, ref, dev):
        return remote(ref, ref, n_s.at[n], n_r.at[n], dev)

    xl, xr, xf = wrap(x - 1, NX), wrap(x + 1, NX), wrap(x + 2, NX)
    n_out = [
        ncopy(0, nbuf.at[x], right_x),
        ncopy(1, nbuf.at[x], left_x),
        ncopy(2, nbuf.at[xl, pl.ds(0, 16)], right_x),
        ncopy(3, nbuf.at[xr, pl.ds(16, 16)], left_x),
    ]
    n_in = [
        ncopy(0, nbuf.at[xl], right_x),
        ncopy(1, nbuf.at[xr], left_x),
        ncopy(2, nbuf.at[xf, pl.ds(0, 16)], right_x),
        ncopy(3, nbuf.at[xf, pl.ds(16, 16)], left_x),
    ]
    n_out[0].start()
    n_out[1].start()
    pump(6)
    pump(7)
    n_in[0].wait_recv()
    n_out[2].start()
    n_in[1].wait_recv()
    n_out[3].start()
    for p in range(8, 15):
        pump(p)
    n_in[2].wait_recv()
    n_in[3].wait_recv()
    normed = nbuf[...].reshape(NX * ROWS, D)

    def all_of(m):
        return remote(w.at[m], wp.at[m], wr_s.at[m], wr_r.at[m], partner)

    def hidden_of(buf):
        gate_part = jnp.dot(normed, buf[0].reshape(D, FFD), preferred_element_type=F32)
        lifted = jnp.dot(normed, buf[1].reshape(D, FFD), preferred_element_type=F32)
        return (gate_part / (1.0 + jnp.exp(-gate_part)) * lifted).astype(BF16)

    hidden = hidden_of(w)
    all_of(0).wait_recv()
    all_of(1).wait_recv()
    hidden_p = hidden_of(wp)
    all_of(2).wait_recv()
    parts = lax.dot_general(hidden, w[2].reshape(D, FFD), NT, preferred_element_type=F32)
    parts = parts + lax.dot_general(hidden_p, wp[2].reshape(D, FFD), NT, preferred_element_type=F32)
    parts = parts.reshape(NX, ROWS, D)
    psend[...] = parts.astype(BF16)
    pown[...] = parts

    def pcopy(d):
        i = wrap(x + d, NX)
        return remote(psend.at[i], precv.at[x], p_s.at[d - 1], p_r.at[d - 1], {"x": i})

    def pcopy_in(d):
        ref = precv.at[wrap(x - d, NX)]
        return remote(ref, ref, p_s.at[d - 1], p_r.at[d - 1], {"x": x})

    for d in (2, 1, 3):
        pcopy(d).start()

    def drain(d):
        for h in range(2):
            kva(h, d).wait_send()
            wa(h, d).wait_send()
        ocopy(d).wait_send()

    each(drain)
    for d in range(1, TEAM):
        qcopy(d).wait_send()
    for copy in ow_out + n_out:
        copy.wait_send()
    for k in range(1, 5):
        for h, d, m in kv_steps(k):
            kvb(h, d, k, m, False).wait_send()
        for h in range(2):
            for d in range(2):
                for m in range(3):
                    wb(h, d, k, m, False).wait_send()
    for m in range(3):
        all_of(m).wait_send()

    total = mid[...].astype(F32) + pown[x]
    for d in (1, 3, 2):
        pcopy_in(d).wait_recv()
        total = total + precv[wrap(x - d, NX)].astype(F32)
    out_ref[...] = total.astype(BF16)
    for d in range(1, NX):
        pcopy(d).wait_send()


def local(
    queries, keys, values, query_gain, key_gain, residual_in, out_weight, norm_gain,
    gate_weight, up_weight, down_weight,
):
    vmem = pl.BlockSpec(memory_space=pltpu.VMEM)
    dma = pltpu.SemaphoreType.DMA
    tables = [jnp.asarray(t) for t in rope_tables()]
    return pl.pallas_call(
        layer_kernel,
        name="layer",
        out_shape=jax.ShapeDtypeStruct((ROWS, D), BF16),
        in_specs=[vmem] * 6 + [pl.BlockSpec(memory_space=pl.ANY)] + [vmem] * 8,
        out_specs=vmem,
        scratch_shapes=[
            pltpu.VMEM((TEAM, TOK, HEAD), BF16),
            pltpu.VMEM((NZ, 2, NY, KH, HEAD), BF16),
            pltpu.VMEM((NY, 2, NZ, KH, HEAD), BF16),
            pltpu.VMEM((3, NZ, NY, 2, 16, FFD), BF16),
            pltpu.VMEM((3, NZ, NY, 2, 16, FFD), BF16),
            pltpu.VMEM((8, HEAD, D), BF16),
            pltpu.VMEM((TEAM, TOK, 2 * HEAD), F32),
            pltpu.VMEM((TEAM, TOK, HEAD), F32),
            pltpu.VMEM((8, ROWS, (TEAM + 1) * HEAD), BF16),
            pltpu.VMEM((8, ROWS, (TEAM + 1) * HEAD), BF16),
            pltpu.VMEM((ROWS, 8 * HEAD), BF16),
            pltpu.VMEM((NX, ROWS, D), BF16),
            pltpu.VMEM((ROWS, D), BF16),
            pltpu.VMEM((NX, ROWS, D), BF16),
            pltpu.VMEM((NX, ROWS, D), F32),
            pltpu.VMEM((NX, ROWS, D), BF16),
            dma((3,)), dma((3,)),
            dma((2, 7)), dma((2, 7)),
            dma((2, 7)), dma((2, 7)),
            dma((2, 2, 4, 2)), dma((2, 2, 4, 2)),
            dma((2, 2, 4, 3)), dma((2, 2, 4, 3)),
            dma((3,)), dma((3,)),
            dma, dma((9,)), dma((9,)),
            dma((7,)), dma((7,)),
            dma((4,)), dma((4,)),
            dma((3,)), dma((3,)),
        ],
        compiler_params=pltpu.CompilerParams(
            collective_id=0, has_side_effects=True, vmem_limit_bytes=56 * 1024 * 1024
        ),
    )(
        queries, keys, values, query_gain.reshape(1, -1), key_gain.reshape(1, -1), residual_in,
        out_weight, norm_gain.reshape(1, -1), gate_weight, up_weight, down_weight, *tables,
    )


def solution(mesh):
    finer = Mesh(mesh.devices.reshape(NZ, NY, NX, 2), ("z", "y", "x", "c"))
    sp, tp = ("z", "y"), ("x", "c")
    in_specs = (
        P(sp, tp),
        P(sp, None),
        P(sp, None),
        P(),
        P(),
        P(sp + tp, None),
        P(tp, None),
        P(),
        P(sp, tp),
        P(sp, tp),
        P(tp, sp),
    )
    return jax.shard_map(
        local, mesh=finer, in_specs=in_specs, out_specs=P(sp + tp, None), check_vma=False
    )
```

```python
import math

import jax
import jax.numpy as jnp
import numpy as np
from jax import lax
from jax.experimental import pallas as pl
from jax.experimental.pallas import tpu as pltpu
from jax.sharding import Mesh
from jax.sharding import PartitionSpec as P

NZ = 8
NY = 8
RING = 8
NX = 4
HEAD = 128
GRID_WIDTH = 64
TOK = 256
TEAM = 4
KTOK = TOK // TEAM
KH = KTOK // 2
ROWS = 32
D = 2048
FFD = 384
EPS = 1e-06
ROPE_BASE = 10000.0
SCALE = HEAD ** (-0.5) * math.log2(math.e)
F32 = jnp.float32
BF16 = jnp.bfloat16
NT = (((1,), (1,)), ((), ()))
FAR_FIRST = (4, 3, 5, 2, 6, 1, 7)


def rope_tables():
    quarter = HEAD // 4
    inverse = ROPE_BASE ** (-np.arange(quarter, dtype=np.float64) * 2.0 / (HEAD // 2))
    rows = np.arange(NZ * NY * TOK // GRID_WIDTH, dtype=np.float64)[:, None] * inverse
    cols = np.arange(GRID_WIDTH, dtype=np.float64)[:, None] * inverse

    def half(angles):
        return (
            np.concatenate([np.cos(angles), np.cos(angles)], axis=1),
            np.concatenate([-np.sin(angles), np.sin(angles)], axis=1),
        )

    rc, rs = half(rows)
    cc, cs = half(cols)
    rc, rs = rc.reshape(-1, 4, HEAD // 2), rs.reshape(-1, 4, HEAD // 2)
    left = lambda a: np.concatenate([a, np.zeros_like(a)], axis=-1).astype(np.float32)
    right = lambda a: np.concatenate([np.zeros_like(a), a], axis=-1).astype(np.float32)
    return np.stack([left(rc), left(rs)], axis=1), np.stack([right(cc), right(cs)])


def normalize(x, gain):
    return x * lax.rsqrt(jnp.mean(x * x, axis=-1, keepdims=True) + EPS) * gain


def turn(x, cosine, sine):
    lane = lax.broadcasted_iota(jnp.int32, x.shape, 1)
    ahead = pltpu.roll(x, HEAD - 32, 1)
    behind = pltpu.roll(x, 32, 1)
    partner = jnp.where((lane // 32) % 2 == 0, ahead, behind)
    return x * cosine + partner * sine


def layer_kernel(
    q_hbm, k_hbm, v_hbm, qg_hbm, kg_hbm, res_hbm, ow_hbm, ng_hbm, gate_hbm, up_hbm, down_hbm,
    row_hbm, col_hbm,
    out_ref,
    q_ref, k_ref, qg_ref, kg_ref, res_ref, ng_ref, row_ref, col_ref,
    qbuf, kv0, kv1, w, wp, ow, acc, peak, osend, orecv, att, nbuf, mid, psend, pown, precv, pfar, pmix,
    in_s, q_s, q_r, ka_s, ka_r, wa_s, wa_r, kb_s, kb_r, wb_s, wb_r, wr_s, wr_r,
    ow_s, ow_r, o_s, o_r, n_s, n_r, p_s, p_r,
):
    z = lax.axis_index("z")
    y = lax.axis_index("y")
    x = lax.axis_index("x")
    c = lax.axis_index("c")
    tp = x * 2 + c
    team = x // 2
    j = lax.rem(x, 2) * 2 + c
    s = z * NY + y
    pos = (z, y)
    axis = ("z", "y")

    def wrap(v, n=RING):
        return lax.rem(v + n, n)

    def tp_id(i):
        return {"x": i // 2, "c": lax.rem(i, 2)}

    barrier = pltpu.get_barrier_semaphore()

    def greet(d, carry):
        pl.semaphore_signal(barrier, inc=1, device_id={"z": wrap(z + d)})
        pl.semaphore_signal(barrier, inc=1, device_id={"y": wrap(y + d)})
        pl.semaphore_signal(barrier, inc=1, device_id=tp_id(wrap(tp + d)))
        return carry

    lax.fori_loop(1, RING, greet, 0)

    lanes = pl.ds(pl.multiple_of(team * HEAD, HEAD), HEAD)

    def key_rows(half):
        return pl.ds(pl.multiple_of(j * KTOK + half * KH, KH), KH)

    loads = [
        (k_hbm.at[pl.ds(pl.multiple_of(j * KTOK, KTOK), KTOK), lanes], k_ref),
        (row_hbm.at[s], row_ref),
        (col_hbm, col_ref),
        (kg_hbm, kg_ref),
        (q_hbm, q_ref),
        (qg_hbm, qg_ref),
        (ow_hbm, ow.at[tp]),
        (res_hbm, res_ref),
        (ng_hbm, ng_ref),
        (v_hbm.at[key_rows(0), lanes], kv0.at[z, 1, y]),
        (v_hbm.at[key_rows(1), lanes], kv1.at[y, 1, z]),
        (gate_hbm, w.at[0, z, y]),
        (up_hbm, w.at[1, z, y]),
        (down_hbm, w.at[2, z, y]),
    ]
    sems = [in_s.at[n] for n in (0, 1, 2, 3, 4, 5, 6, 7, 8, 9, 9, 10, 10, 10)]
    loads = [pltpu.make_async_copy(a, b, m) for (a, b), m in zip(loads, sems)]

    def landed(ref, sem):
        pltpu.make_async_copy(ref, ref, sem).wait()

    for load in loads:
        load.start()

    for load in loads[:4]:
        load.wait()
    cosine = row_ref[0, pl.ds(j, 1), :] + col_ref[0]
    sine = row_ref[1, pl.ds(j, 1), :] + col_ref[1]
    kk = k_ref[...].astype(F32)
    kk = turn(normalize(kk, kg_ref[...]), cosine, sine).astype(BF16)
    kv0[z, 0, y] = kk[:KH]
    kv1[y, 0, z] = kk[KH:]
    landed(kv0.at[z, 1, 0:2], in_s.at[9])
    pl.semaphore_wait(barrier, 21)

    partner = {"c": 1 - c}

    def remote(ref, dst, ss, rs, dev):
        return pltpu.make_async_remote_copy(
            src_ref=ref, dst_ref=dst, send_sem=ss, recv_sem=rs,
            device_id=dev, device_id_type=pl.DeviceIdType.MESH,
        )

    def arrived(ref, sem):
        remote(ref, ref, sem, sem, partner).wait_recv()

    def sent(ref, sem):
        remote(ref, ref, sem, sem, partner).wait_send()

    def kva(h, d):
        ref = kv0.at[z, :, y] if h == 0 else kv1.at[y, :, z]
        dev = {"y": wrap(y + d)} if h == 0 else {"z": wrap(z + d)}
        return remote(ref, ref, ka_s.at[h], ka_r.at[h], dev)

    def wa(h, d, part):
        pick = slice(0, 2) if part == 0 else slice(2, 3)
        ref = w.at[pick, z, y, h]
        dev = {"y": wrap(y + d)} if h == 0 else {"z": wrap(z + d)}
        return remote(ref, ref, wa_s.at[h], wa_r.at[part, h], dev)

    def w_first(part):
        for d in FAR_FIRST:
            wa(0, d, part).start()
            wa(1, d, part).start()

    def w_first_in(part):
        pick = slice(0, 2) if part == 0 else slice(2, 3)
        arrived(w.at[pick, z, 0:7, 0], wa_r.at[part, 0])
        arrived(w.at[pick, 0:7, y, 1], wa_r.at[part, 1])

    def start_kva(d):
        kva(0, d).start()
        kva(1, d).start()

    for d in FAR_FIRST:
        start_kva(d)
    landed(w.at[:, z, y], in_s.at[10])
    w_first(0)

    loads[4].wait()
    loads[5].wait()
    for r in range(4):
        part = slice(r * GRID_WIDTH, (r + 1) * GRID_WIDTH)
        cosine = row_ref[0, r : r + 1, :] + col_ref[0]
        sine = row_ref[1, r : r + 1, :] + col_ref[1]
        qq = turn(normalize(q_ref[part, :].astype(F32), qg_ref[...]), cosine, sine)
        qbuf[j, part] = (qq * SCALE).astype(BF16)
    peak[...] = jnp.full(peak.shape, -1e30, F32)
    acc[...] = jnp.zeros(acc.shape, F32)

    def qcopy(d):
        other = team * TEAM + lax.rem(j + d, TEAM)
        return remote(qbuf.at[j], qbuf.at[j], q_s, q_r, tp_id(other))

    for d in range(1, TEAM):
        qcopy(d).start()

    right_x = {"x": wrap(x + 1, NX)}
    left_x = {"x": wrap(x - 1, NX)}
    tl = wrap(x - 1, NX) * 2 + c
    tr = wrap(x + 1, NX) * 2 + c
    far = wrap(x + 2, NX) * 2 + c

    def head_ref(i, part=None):
        if part is None:
            return ow.at[i]
        return ow.at[i, pl.ds(part * 64, 64)]

    def owcopy(n, ref, dev):
        return remote(ref, ref, ow_s, ow_r.at[n], dev)

    ow_out = [
        owcopy(0, head_ref(tp), right_x),
        owcopy(1, head_ref(tp), left_x),
        owcopy(4, head_ref(tp), partner),
        owcopy(2, head_ref(tl, 0), right_x),
        owcopy(3, head_ref(tr, 1), left_x),
        owcopy(4, head_ref(tl), partner),
        owcopy(4, head_ref(tr), partner),
        owcopy(4, head_ref(far, 0), partner),
        owcopy(4, head_ref(far, 1), partner),
    ]
    ow_in = [
        owcopy(0, head_ref(tl), right_x),
        owcopy(1, head_ref(tr), left_x),
        owcopy(2, head_ref(far, 0), right_x),
        owcopy(3, head_ref(far, 1), left_x),
    ]
    loads[6].wait()

    for n in range(3):
        ow_out[n].start()

    def kvb(h, d, k, m):
        shift = (k - 1) * (-1 if d == 0 else 1)
        buf = kv0 if h == 0 else kv1
        ref = buf.at[wrap(pos[h] + shift), m]
        dev = {axis[h]: wrap(pos[h] + (1 if d == 0 else -1))}
        return remote(ref, ref, kb_s.at[h], kb_r.at[k - 1], dev)

    def kv_steps(k):
        return [(h, d, m) for m in range(2) for h in range(2) for d in range(2) if k < 4 or d == m]

    def kv_send(k):
        if k > 1:
            arrived(kv0.at[0:4], kb_r.at[k - 2])
        for h, d, m in kv_steps(k):
            kvb(h, d, k, m).start()

    def w_block(h, b, m, lo, hi):
        if h == 0:
            return lambda buf: buf.at[m, b, lo:hi, 0]
        return lambda buf: buf.at[m, lo:hi, b, 1]

    def wb(h, d, k, m):
        shift = (k - 1) * (-1 if d == 0 else 1)
        lo, hi = (0, RING) if k < 4 else ((0, 4) if d == 0 else (4, RING))
        ref = w_block(h, wrap(pos[h] + shift), m, lo, hi)(w)
        dev = {axis[h]: wrap(pos[h] + (1 if d == 0 else -1))}
        return remote(ref, ref, wb_s, wb_r.at[k - 1, m], dev)

    def hand_over(h, d, k, m):
        shift = k * (-1 if d == 0 else 1)
        lo, hi = (0, RING) if k < 4 else ((0, 4) if d == 0 else (4, RING))
        pick = w_block(h, wrap(pos[h] + shift), m, lo, hi)
        remote(pick(w), pick(wp), wr_s, wr_r.at[m], partner).start()

    def pump(k, m):
        if k > 1:
            arrived(w.at[m, 0 : 2 if k < 5 else 1], wb_r.at[k - 2, m])
        if k <= 4:
            for h in range(2):
                for d in range(2):
                    wb(h, d, k, m).start()
        for h in range(2):
            for d in range(2):
                if k > 1:
                    hand_over(h, d, k - 1, m)
                elif d == 0:
                    hand_over(h, 0, 0, m)

    ones = jnp.ones((1, HEAD), BF16)

    def attend(blocks):
        keys = jnp.concatenate([buf[b, 0].reshape(256, HEAD) for buf, b in blocks], axis=0)
        vals = jnp.concatenate([buf[b, 1].reshape(256, HEAD) for buf, b in blocks], axis=0)
        wide = keys.shape[0]
        vals = jnp.concatenate([vals, jnp.broadcast_to(ones, vals.shape)], axis=1)

        def scores_of(h):
            return lax.dot_general(qbuf[h], keys, NT, preferred_element_type=F32)

        scores = scores_of(0)
        for h in range(TEAM):
            later = scores_of(h + 1) if h + 1 < TEAM else None
            old = peak[h]
            new = jnp.maximum(old, jnp.max(scores, axis=1, keepdims=True))
            factor = jnp.exp2(old - new)
            peak[h] = new
            raw = jnp.exp2(scores - jnp.concatenate([new] * (wide // HEAD), axis=1)).astype(BF16)
            update = jnp.dot(raw, vals, preferred_element_type=F32)
            acc[h] = acc[h] * jnp.concatenate([factor, factor], axis=1) + update
            scores = later

    arrived(kv0.at[0, :, 0:7], ka_r.at[0])
    arrived(kv0.at[0, :, 0:7], ka_r.at[1])
    kv_send(1)
    arrived(qbuf.at[0:3], q_r)
    w_first_in(0)
    pump(1, 0)
    attend([(kv0, z), (kv1, y)])
    kv_send(2)
    pump(1, 1)
    w_first(1)
    attend([(kv0, wrap(z - 1)), (kv0, wrap(z + 1)), (kv1, wrap(y - 1)), (kv1, wrap(y + 1))])
    kv_send(3)
    pump(2, 0)
    ow_in[0].wait_recv()
    ow_out[3].start()
    ow_in[1].wait_recv()
    ow_out[4].start()
    ow_out[5].start()
    ow_out[6].start()
    attend([(kv0, wrap(z - 2)), (kv0, wrap(z + 2)), (kv1, wrap(y - 2)), (kv1, wrap(y + 2))])
    kv_send(4)
    pump(2, 1)
    attend([(kv0, wrap(z - 3)), (kv0, wrap(z + 3)), (kv1, wrap(y - 3)), (kv1, wrap(y + 3))])
    w_first_in(1)
    pump(1, 2)
    arrived(kv0.at[0:2], kb_r.at[3])
    attend([(kv0, wrap(z + 4)), (kv1, wrap(y + 4))])
    pump(3, 0)

    lane = lax.broadcasted_iota(jnp.int32, (TOK, HEAD), 1)
    stats = jnp.zeros((TOK, HEAD), F32)
    for h in range(TEAM):
        total = acc[h, :, HEAD:]
        mean = (acc[h, :, :HEAD] / total).astype(BF16)
        osend[:, :, h * HEAD : (h + 1) * HEAD] = mean.reshape(8, ROWS, HEAD)
        level = peak[h] + jnp.log2(total)
        first = level.astype(BF16).astype(F32)
        second = (level - first).astype(BF16).astype(F32)
        third = level - first - second
        stats = jnp.where(lane == h, first, stats)
        stats = jnp.where(lane == h + 4, second, stats)
        stats = jnp.where(lane == h + 8, third, stats)
    osend[:, :, TEAM * HEAD :] = stats.astype(BF16).reshape(8, ROWS, HEAD)

    def ocopy(d):
        i = wrap(tp + d)
        return remote(osend.at[i], orecv.at[tp], o_s, o_r, tp_id(i))

    for d in (4, 3, 5, 2, 6, 1, 7):
        ocopy(d).start()
    orecv[tp] = osend[tp]

    pump(3, 1)
    ow_in[2].wait_recv()
    ow_out[7].start()
    ow_in[3].wait_recv()
    ow_out[8].start()
    pump(2, 2)

    arrived(orecv.at[0:7], o_r)
    for t in range(2):
        for h in range(TEAM):
            levels = []
            for i in range(t * TEAM, (t + 1) * TEAM):
                st = orecv[i, :, TEAM * HEAD :].astype(F32)
                levels.append(st[:, h : h + 1] + st[:, h + 4 : h + 5] + st[:, h + 8 : h + 9])
            top = jnp.maximum(jnp.maximum(levels[0], levels[1]), jnp.maximum(levels[2], levels[3]))
            shares = [jnp.exp2(v - top) for v in levels]
            total = shares[0] + shares[1] + shares[2] + shares[3]
            mixed = jnp.zeros((ROWS, HEAD), F32)
            for i in range(TEAM):
                block = orecv[t * TEAM + i, :, h * HEAD : (h + 1) * HEAD].astype(F32)
                mixed = mixed + block * shares[i]
            at = (t * TEAM + h) * HEAD
            att[:, at : at + HEAD] = (mixed / total).astype(BF16)

    arrived(ow.at[0:4], ow_r.at[4])
    loads[7].wait()
    loads[8].wait()
    projected = jnp.dot(att[...], ow[...].reshape(8 * HEAD, D), preferred_element_type=F32)
    middle = (res_ref[...].astype(F32) + projected).astype(BF16)
    mid[...] = middle
    nbuf[x] = normalize(middle.astype(F32), ng_ref[...]).astype(BF16)

    def ncopy(n, ref, dev):
        return remote(ref, ref, n_s, n_r.at[min(n, 2)], dev)

    xl, xr, xf = wrap(x - 1, NX), wrap(x + 1, NX), wrap(x + 2, NX)
    low, high = pl.ds(0, 16), pl.ds(16, 16)
    n_out = [
        ncopy(0, nbuf.at[x, low], right_x),
        ncopy(1, nbuf.at[x, high], left_x),
        ncopy(2, nbuf.at[x, high], right_x),
        ncopy(3, nbuf.at[x, low], left_x),
        ncopy(4, nbuf.at[xl, low], right_x),
        ncopy(5, nbuf.at[xr, high], left_x),
    ]
    n_in = [
        ncopy(0, nbuf.at[xl, low], right_x),
        ncopy(1, nbuf.at[xr, high], left_x),
    ]
    for copy in n_out[:4]:
        copy.start()
    pump(4, 0)
    n_in[0].wait_recv()
    n_out[4].start()
    n_in[1].wait_recv()
    n_out[5].start()
    pump(4, 1)
    pump(3, 2)
    pump(5, 0)
    pump(5, 1)
    arrived(nbuf.at[0:2], n_r.at[2])
    normed = nbuf[...].reshape(NX * ROWS, D)

    def all_of(m):
        return remote(w.at[m], wp.at[m], wr_s, wr_r.at[m], partner)

    def hidden_of(buf):
        gate_part = jnp.dot(normed, buf[0].reshape(D, FFD), preferred_element_type=F32)
        lifted = jnp.dot(normed, buf[1].reshape(D, FFD), preferred_element_type=F32)
        return (gate_part / (1.0 + jnp.exp(-gate_part)) * lifted).astype(BF16)

    hidden = hidden_of(w)
    pump(4, 2)
    all_of(0).wait_recv()
    all_of(1).wait_recv()
    hidden_p = hidden_of(wp)
    pump(5, 2)
    all_of(2).wait_recv()
    parts = lax.dot_general(hidden, w[2].reshape(D, FFD), NT, preferred_element_type=F32)
    parts = parts + lax.dot_general(hidden_p, wp[2].reshape(D, FFD), NT, preferred_element_type=F32)
    parts = parts.reshape(NX, ROWS, D)
    psend[...] = parts.astype(BF16)
    pown[...] = parts

    def pcopy(n, src, dst, dev):
        return remote(src, dst, p_s, p_r.at[min(n, 2)], dev)

    p_copies = [
        pcopy(0, psend.at[xf, low], pfar.at[0], right_x),
        pcopy(1, psend.at[xf, high], pfar.at[1], left_x),
        pcopy(2, psend.at[xr, high], precv.at[0, high], right_x),
        pcopy(3, psend.at[xl, low], precv.at[1, low], left_x),
        pcopy(4, pmix.at[0], precv.at[0, low], right_x),
        pcopy(5, pmix.at[1], precv.at[1, high], left_x),
    ]
    for copy in p_copies[:4]:
        copy.start()
    p_copies[0].wait_recv()
    pmix[0] = (pown[xr, low] + pfar[0].astype(F32)).astype(BF16)
    p_copies[4].start()
    p_copies[1].wait_recv()
    pmix[1] = (pown[xl, high] + pfar[1].astype(F32)).astype(BF16)
    p_copies[5].start()

    def drain():
        for h in range(2):
            sent(kv0.at[0, :, 0:7], ka_s.at[h])
            sent(w.at[:, z, 0:7, 0], wa_s.at[h])
            sent(kv0.at[0:7], kb_s.at[h])
        sent(qbuf.at[0:3], q_s)
        sent(osend.at[0:7], o_s)
        sent(ow.at[0:7], ow_s)
        sent(nbuf.at[0:3], n_s)
        sent(w.at[:, 0:7], wb_s)
        sent(w, wr_s)

    def finish():
        total = mid[...].astype(F32) + pown[x] + precv[0].astype(F32) + precv[1].astype(F32)
        out_ref[...] = total.astype(BF16)
        sent(psend.at[0:3], p_s)

    drain()
    arrived(precv, p_r.at[2])
    finish()


def local(
    queries, keys, values, query_gain, key_gain, residual_in, out_weight, norm_gain,
    gate_weight, up_weight, down_weight,
):
    vmem = pl.BlockSpec(memory_space=pltpu.VMEM)
    dma = pltpu.SemaphoreType.DMA
    tables = [jnp.asarray(t) for t in rope_tables()]
    return pl.pallas_call(
        layer_kernel,
        name="layer",
        out_shape=jax.ShapeDtypeStruct((ROWS, D), BF16),
        in_specs=[pl.BlockSpec(memory_space=pl.ANY)] * 13,
        out_specs=vmem,
        scratch_shapes=[
            pltpu.VMEM((TOK, HEAD), BF16),
            pltpu.VMEM((KTOK, HEAD), BF16),
            pltpu.VMEM((1, HEAD), F32),
            pltpu.VMEM((1, HEAD), F32),
            pltpu.VMEM((ROWS, D), BF16),
            pltpu.VMEM((1, D), F32),
            pltpu.VMEM((2, 4, HEAD), F32),
            pltpu.VMEM((2, GRID_WIDTH, HEAD), F32),
            pltpu.VMEM((TEAM, TOK, HEAD), BF16),
            pltpu.VMEM((NZ, 2, NY, KH, HEAD), BF16),
            pltpu.VMEM((NY, 2, NZ, KH, HEAD), BF16),
            pltpu.VMEM((3, NZ, NY, 2, 16, FFD), BF16),
            pltpu.VMEM((3, NZ, NY, 2, 16, FFD), BF16),
            pltpu.VMEM((8, HEAD, D), BF16),
            pltpu.VMEM((TEAM, TOK, 2 * HEAD), F32),
            pltpu.VMEM((TEAM, TOK, HEAD), F32),
            pltpu.VMEM((8, ROWS, (TEAM + 1) * HEAD), BF16),
            pltpu.VMEM((8, ROWS, (TEAM + 1) * HEAD), BF16),
            pltpu.VMEM((ROWS, 8 * HEAD), BF16),
            pltpu.VMEM((NX, ROWS, D), BF16),
            pltpu.VMEM((ROWS, D), BF16),
            pltpu.VMEM((NX, ROWS, D), BF16),
            pltpu.VMEM((NX, ROWS, D), F32),
            pltpu.VMEM((2, ROWS, D), BF16),
            pltpu.VMEM((2, 16, D), BF16),
            pltpu.VMEM((2, 16, D), BF16),
            dma((11,)), dma, dma,
            dma((2,)), dma((2,)),
            dma((2,)), dma((2, 2)),
            dma((2,)), dma((4,)),
            dma, dma((4, 3)),
            dma, dma((3,)),
            dma, dma((5,)),
            dma, dma,
            dma, dma((3,)),
            dma, dma((3,)),
        ],
        compiler_params=pltpu.CompilerParams(
            collective_id=0, has_side_effects=True, vmem_limit_bytes=56 * 1024 * 1024
        ),
    )(
        queries, keys, values, query_gain.reshape(1, -1), key_gain.reshape(1, -1), residual_in,
        out_weight, norm_gain.reshape(1, -1),
        *[a.reshape(2, 16, FFD) for a in (gate_weight, up_weight, down_weight.T)], *tables,
    )


def solution(mesh):
    finer = Mesh(mesh.devices.reshape(NZ, NY, NX, 2), ("z", "y", "x", "c"))
    sp, tp = ("z", "y"), ("x", "c")
    in_specs = (
        P(sp, tp),
        P(sp, None),
        P(sp, None),
        P(),
        P(),
        P(sp + tp, None),
        P(tp, None),
        P(),
        P(sp, tp),
        P(sp, tp),
        P(tp, sp),
    )
    return jax.shard_map(
        local, mesh=finer, in_specs=in_specs, out_specs=P(sp + tp, None), check_vma=False
    )
```

```python
import math

import jax
import jax.numpy as jnp
import numpy as np
from jax import lax
from jax.experimental import pallas as pl
from jax.experimental.pallas import tpu as pltpu
from jax.sharding import Mesh
from jax.sharding import PartitionSpec as P

NZ = 8
NY = 8
RING = 8
NX = 4
HEAD = 128
GRID_WIDTH = 64
TOK = 256
TEAM = 4
KTOK = TOK // TEAM
KH = KTOK // 2
ROWS = 32
D = 2048
FFD = 384
EPS = 1e-06
ROPE_BASE = 10000.0
SCALE = HEAD ** (-0.5) * math.log2(math.e)
F32 = jnp.float32
BF16 = jnp.bfloat16
NT = (((1,), (1,)), ((), ()))
FAR_FIRST = (4, 3, 5, 2, 6, 1, 7)


def rope_tables():
    quarter = HEAD // 4
    inverse = ROPE_BASE ** (-np.arange(quarter, dtype=np.float64) * 2.0 / (HEAD // 2))
    rows = np.arange(NZ * NY * TOK // GRID_WIDTH, dtype=np.float64)[:, None] * inverse
    cols = np.arange(GRID_WIDTH, dtype=np.float64)[:, None] * inverse

    def half(angles):
        return (
            np.concatenate([np.cos(angles), np.cos(angles)], axis=1),
            np.concatenate([-np.sin(angles), np.sin(angles)], axis=1),
        )

    rc, rs = half(rows)
    cc, cs = half(cols)
    rc, rs = rc.reshape(-1, 4, HEAD // 2), rs.reshape(-1, 4, HEAD // 2)
    left = lambda a: np.concatenate([a, np.zeros_like(a)], axis=-1).astype(np.float32)
    right = lambda a: np.concatenate([np.zeros_like(a), a], axis=-1).astype(np.float32)
    return np.stack([left(rc), left(rs)], axis=1), np.stack([right(cc), right(cs)])


def normalize(x, gain):
    return x * lax.rsqrt(jnp.mean(x * x, axis=-1, keepdims=True) + EPS) * gain


def turn(x, cosine, sine):
    lane = lax.broadcasted_iota(jnp.int32, x.shape, 1)
    ahead = pltpu.roll(x, HEAD - 32, 1)
    behind = pltpu.roll(x, 32, 1)
    partner = jnp.where((lane // 32) % 2 == 0, ahead, behind)
    return x * cosine + partner * sine


def layer_kernel(
    q_hbm, k_hbm, v_hbm, qg_hbm, kg_hbm, res_hbm, ow_hbm, ng_hbm, gate_hbm, up_hbm, down_hbm,
    row_hbm, col_hbm,
    out_ref,
    q_ref, k_ref, qg_ref, kg_ref, res_ref, ng_ref, row_ref, col_ref,
    qbuf, kv0, kv1, w, wp, ow, acc, peak, osend, orecv, att, nbuf, mid, psend, pown, precv, pfar, pmix,
    in_s, q_s, q_r, ka_s, ka_r, wa_s, wa_r, kb_s, kb_r, wb_s, wb_r, wr_s, wr_r,
    ow_s, ow_r, o_s, o_r, n_s, n_r, p_s, p_r,
):
    z = lax.axis_index("z")
    y = lax.axis_index("y")
    x = lax.axis_index("x")
    c = lax.axis_index("c")
    tp = x * 2 + c
    team = x // 2
    j = lax.rem(x, 2) * 2 + c
    s = z * NY + y
    pos = (z, y)
    axis = ("z", "y")

    def wrap(v, n=RING):
        return lax.rem(v + n, n)

    def tp_id(i):
        return {"x": i // 2, "c": lax.rem(i, 2)}

    barrier = pltpu.get_barrier_semaphore()

    def greet(d, carry):
        pl.semaphore_signal(barrier, inc=1, device_id={"z": wrap(z + d)})
        pl.semaphore_signal(barrier, inc=1, device_id={"y": wrap(y + d)})
        pl.semaphore_signal(barrier, inc=1, device_id=tp_id(wrap(tp + d)))
        return carry

    lax.fori_loop(1, RING, greet, 0)

    lanes = pl.ds(pl.multiple_of(team * HEAD, HEAD), HEAD)

    def key_rows(half):
        return pl.ds(pl.multiple_of(j * KTOK + half * KH, KH), KH)

    loads = [
        (k_hbm.at[pl.ds(pl.multiple_of(j * KTOK, KTOK), KTOK), lanes], k_ref),
        (row_hbm.at[s], row_ref),
        (col_hbm, col_ref),
        (kg_hbm, kg_ref),
        (q_hbm, q_ref),
        (qg_hbm, qg_ref),
        (ow_hbm, ow.at[tp]),
        (res_hbm, res_ref),
        (ng_hbm, ng_ref),
        (v_hbm.at[key_rows(0), lanes], kv0.at[z, 1, y]),
        (v_hbm.at[key_rows(1), lanes], kv1.at[y, 1, z]),
        (gate_hbm, w.at[0, z, y]),
        (up_hbm, w.at[1, z, y]),
        (down_hbm, w.at[2, z, y]),
    ]
    sems = [in_s.at[n] for n in (0, 1, 2, 3, 4, 5, 6, 7, 8, 9, 9, 10, 10, 10)]
    loads = [pltpu.make_async_copy(a, b, m) for (a, b), m in zip(loads, sems)]

    def landed(ref, sem):
        pltpu.make_async_copy(ref, ref, sem).wait()

    for load in loads:
        load.start()

    for load in loads[:4]:
        load.wait()
    cosine = row_ref[0, pl.ds(j, 1), :] + col_ref[0]
    sine = row_ref[1, pl.ds(j, 1), :] + col_ref[1]
    kk = k_ref[...].astype(F32)
    kk = turn(normalize(kk, kg_ref[...]), cosine, sine).astype(BF16)
    kv0[z, 0, y] = kk[:KH]
    kv1[y, 0, z] = kk[KH:]
    landed(kv0.at[z, 1, 0:2], in_s.at[9])
    pl.semaphore_wait(barrier, 21)

    partner = {"c": 1 - c}

    def remote(ref, dst, ss, rs, dev):
        return pltpu.make_async_remote_copy(
            src_ref=ref, dst_ref=dst, send_sem=ss, recv_sem=rs,
            device_id=dev, device_id_type=pl.DeviceIdType.MESH,
        )

    def arrived(ref, sem):
        remote(ref, ref, sem, sem, partner).wait_recv()

    def sent(ref, sem):
        remote(ref, ref, sem, sem, partner).wait_send()

    def kva(h, d):
        ref = kv0.at[z, :, y] if h == 0 else kv1.at[y, :, z]
        dev = {"y": wrap(y + d)} if h == 0 else {"z": wrap(z + d)}
        return remote(ref, ref, ka_s.at[h], ka_r.at[h], dev)

    def wa(h, d, k):
        shift = (k - 1) * (-1 if d == 0 else 1)
        pick = slice(0, 3) if k < 4 else (slice(0, 2) if d == 0 else slice(2, 3))
        ref = w.at[pick, z, wrap(y + shift), 0] if h == 0 else w.at[pick, wrap(z + shift), y, 1]
        step = 1 if d == 0 else -1
        dev = {"y": wrap(y + step)} if h == 0 else {"z": wrap(z + step)}
        return remote(ref, ref, wa_s, wa_r.at[k - 1], dev)

    def w_first(k):
        if k > 1:
            arrived(w.at[:, z, 0 : 4 if k < 5 else 2, 0], wa_r.at[k - 2])
        if k <= 4:
            for h in range(2):
                for d in range(2):
                    wa(h, d, k).start()

    def start_kva(d):
        kva(0, d).start()
        kva(1, d).start()

    landed(w.at[:, z, y], in_s.at[10])
    w_first(1)
    for d in FAR_FIRST:
        start_kva(d)

    loads[4].wait()
    loads[5].wait()
    for r in range(4):
        part = slice(r * GRID_WIDTH, (r + 1) * GRID_WIDTH)
        cosine = row_ref[0, r : r + 1, :] + col_ref[0]
        sine = row_ref[1, r : r + 1, :] + col_ref[1]
        qq = turn(normalize(q_ref[part, :].astype(F32), qg_ref[...]), cosine, sine)
        qbuf[j, part] = (qq * SCALE).astype(BF16)
    peak[...] = jnp.full(peak.shape, -1e30, F32)
    acc[...] = jnp.zeros(acc.shape, F32)

    def qcopy(d):
        other = team * TEAM + lax.rem(j + d, TEAM)
        return remote(qbuf.at[j], qbuf.at[j], q_s, q_r, tp_id(other))

    for d in range(1, TEAM):
        qcopy(d).start()

    right_x = {"x": wrap(x + 1, NX)}
    left_x = {"x": wrap(x - 1, NX)}
    tl = wrap(x - 1, NX) * 2 + c
    tr = wrap(x + 1, NX) * 2 + c
    far = wrap(x + 2, NX) * 2 + c

    def head_ref(i, part=None):
        if part is None:
            return ow.at[i]
        return ow.at[i, pl.ds(part * 64, 64)]

    def owcopy(n, ref, dev):
        return remote(ref, ref, ow_s, ow_r.at[n], dev)

    ow_out = [
        owcopy(0, head_ref(tp), right_x),
        owcopy(1, head_ref(tp), left_x),
        owcopy(4, head_ref(tp), partner),
        owcopy(2, head_ref(tl, 0), right_x),
        owcopy(3, head_ref(tr, 1), left_x),
        owcopy(4, head_ref(tl), partner),
        owcopy(4, head_ref(tr), partner),
        owcopy(4, head_ref(far, 0), partner),
        owcopy(4, head_ref(far, 1), partner),
    ]
    ow_in = [
        owcopy(0, head_ref(tl), right_x),
        owcopy(1, head_ref(tr), left_x),
        owcopy(2, head_ref(far, 0), right_x),
        owcopy(3, head_ref(far, 1), left_x),
    ]
    loads[6].wait()

    for n in range(3):
        ow_out[n].start()

    def kvb(h, d, k, m):
        shift = (k - 1) * (-1 if d == 0 else 1)
        buf = kv0 if h == 0 else kv1
        ref = buf.at[wrap(pos[h] + shift), m]
        dev = {axis[h]: wrap(pos[h] + (1 if d == 0 else -1))}
        return remote(ref, ref, kb_s.at[h], kb_r.at[k - 1, m], dev)

    def kv_pass(k, m):
        if k > 1:
            arrived(kv0.at[0 : 2 if k < 5 else 1], kb_r.at[k - 2, m])
        if k <= 4:
            for h in range(2):
                for d in range(2):
                    if k < 4 or d == m:
                        kvb(h, d, k, m).start()

    def w_block(h, b, m, lo, hi):
        if h == 0:
            return lambda buf: buf.at[m, b, lo:hi, 0]
        return lambda buf: buf.at[m, lo:hi, b, 1]

    def wb(h, d, k, m):
        shift = (k - 1) * (-1 if d == 0 else 1)
        lo, hi = (0, RING) if k < 4 else ((0, 4) if d == 0 else (4, RING))
        ref = w_block(h, wrap(pos[h] + shift), m, lo, hi)(w)
        dev = {axis[h]: wrap(pos[h] + (1 if d == 0 else -1))}
        return remote(ref, ref, wb_s, wb_r.at[k - 1, m], dev)

    def hand_over(h, d, k, m):
        shift = k * (-1 if d == 0 else 1)
        lo, hi = (0, RING) if k < 4 else ((0, 4) if d == 0 else (4, RING))
        pick = w_block(h, wrap(pos[h] + shift), m, lo, hi)
        remote(pick(w), pick(wp), wr_s, wr_r.at[m], partner).start()

    def pump(k, m):
        if k > 1:
            arrived(w.at[m, 0 : 2 if k < 5 else 1], wb_r.at[k - 2, m])
        if k <= 4:
            for h in range(2):
                for d in range(2):
                    wb(h, d, k, m).start()
        for h in range(2):
            for d in range(2):
                if k > 1:
                    hand_over(h, d, k - 1, m)
                elif d == 0:
                    hand_over(h, 0, 0, m)

    ones = jnp.ones((1, HEAD), BF16)

    def attend(blocks):
        keys = jnp.concatenate([buf[b, 0].reshape(256, HEAD) for buf, b in blocks], axis=0)
        vals = jnp.concatenate([buf[b, 1].reshape(256, HEAD) for buf, b in blocks], axis=0)
        wide = keys.shape[0]
        vals = jnp.concatenate([vals, jnp.broadcast_to(ones, vals.shape)], axis=1)

        def scores_of(h):
            return lax.dot_general(qbuf[h], keys, NT, preferred_element_type=F32)

        scores = scores_of(0)
        for h in range(TEAM):
            later = scores_of(h + 1) if h + 1 < TEAM else None
            old = peak[h]
            new = jnp.maximum(old, jnp.max(scores, axis=1, keepdims=True))
            factor = jnp.exp2(old - new)
            peak[h] = new
            raw = jnp.exp2(scores - jnp.concatenate([new] * (wide // HEAD), axis=1)).astype(BF16)
            update = jnp.dot(raw, vals, preferred_element_type=F32)
            acc[h] = acc[h] * jnp.concatenate([factor, factor], axis=1) + update
            scores = later

    w_first(2)
    arrived(kv0.at[0, :, 0:7], ka_r.at[0])
    arrived(kv0.at[0, :, 0:7], ka_r.at[1])
    w_first(3)
    kv_pass(1, 0)
    kv_pass(1, 1)
    arrived(qbuf.at[0:3], q_r)
    attend([(kv0, z), (kv1, y)])
    w_first(4)
    kv_pass(2, 0)
    kv_pass(2, 1)
    attend([(kv0, wrap(z - 1)), (kv0, wrap(z + 1)), (kv1, wrap(y - 1)), (kv1, wrap(y + 1))])
    w_first(5)
    pump(1, 0)
    kv_pass(3, 0)
    kv_pass(3, 1)
    pump(1, 1)
    ow_in[0].wait_recv()
    ow_out[3].start()
    ow_in[1].wait_recv()
    ow_out[4].start()
    ow_out[5].start()
    ow_out[6].start()
    attend([(kv0, wrap(z - 2)), (kv0, wrap(z + 2)), (kv1, wrap(y - 2)), (kv1, wrap(y + 2))])
    kv_pass(4, 0)
    kv_pass(4, 1)
    pump(1, 2)
    attend([(kv0, wrap(z - 3)), (kv0, wrap(z + 3)), (kv1, wrap(y - 3)), (kv1, wrap(y + 3))])
    pump(2, 0)
    kv_pass(5, 0)
    kv_pass(5, 1)
    attend([(kv0, wrap(z + 4)), (kv1, wrap(y + 4))])
    pump(2, 1)

    lane = lax.broadcasted_iota(jnp.int32, (TOK, HEAD), 1)
    stats = jnp.zeros((TOK, HEAD), F32)
    for h in range(TEAM):
        total = acc[h, :, HEAD:]
        mean = (acc[h, :, :HEAD] / total).astype(BF16)
        osend[:, :, h * HEAD : (h + 1) * HEAD] = mean.reshape(8, ROWS, HEAD)
        level = peak[h] + jnp.log2(total)
        first = level.astype(BF16).astype(F32)
        second = (level - first).astype(BF16).astype(F32)
        third = level - first - second
        stats = jnp.where(lane == h, first, stats)
        stats = jnp.where(lane == h + 4, second, stats)
        stats = jnp.where(lane == h + 8, third, stats)
    osend[:, :, TEAM * HEAD :] = stats.astype(BF16).reshape(8, ROWS, HEAD)

    def ocopy(d):
        i = wrap(tp + d)
        return remote(osend.at[i], orecv.at[tp], o_s, o_r, tp_id(i))

    for d in (4, 3, 5, 2, 6, 1, 7):
        ocopy(d).start()
    orecv[tp] = osend[tp]

    pump(2, 2)
    ow_in[2].wait_recv()
    ow_out[7].start()
    ow_in[3].wait_recv()
    ow_out[8].start()
    pump(3, 0)

    arrived(orecv.at[0:7], o_r)
    for t in range(2):
        for h in range(TEAM):
            levels = []
            for i in range(t * TEAM, (t + 1) * TEAM):
                st = orecv[i, :, TEAM * HEAD :].astype(F32)
                levels.append(st[:, h : h + 1] + st[:, h + 4 : h + 5] + st[:, h + 8 : h + 9])
            top = jnp.maximum(jnp.maximum(levels[0], levels[1]), jnp.maximum(levels[2], levels[3]))
            shares = [jnp.exp2(v - top) for v in levels]
            total = shares[0] + shares[1] + shares[2] + shares[3]
            mixed = jnp.zeros((ROWS, HEAD), F32)
            for i in range(TEAM):
                block = orecv[t * TEAM + i, :, h * HEAD : (h + 1) * HEAD].astype(F32)
                mixed = mixed + block * shares[i]
            at = (t * TEAM + h) * HEAD
            att[:, at : at + HEAD] = (mixed / total).astype(BF16)

    arrived(ow.at[0:4], ow_r.at[4])
    loads[7].wait()
    loads[8].wait()
    projected = jnp.dot(att[...], ow[...].reshape(8 * HEAD, D), preferred_element_type=F32)
    middle = (res_ref[...].astype(F32) + projected).astype(BF16)
    mid[...] = middle
    nbuf[x] = normalize(middle.astype(F32), ng_ref[...]).astype(BF16)

    def ncopy(n, ref, dev):
        return remote(ref, ref, n_s, n_r.at[min(n, 2)], dev)

    xl, xr, xf = wrap(x - 1, NX), wrap(x + 1, NX), wrap(x + 2, NX)
    low, high = pl.ds(0, 16), pl.ds(16, 16)
    n_out = [
        ncopy(0, nbuf.at[x, low], right_x),
        ncopy(1, nbuf.at[x, high], left_x),
        ncopy(2, nbuf.at[x, high], right_x),
        ncopy(3, nbuf.at[x, low], left_x),
        ncopy(4, nbuf.at[xl, low], right_x),
        ncopy(5, nbuf.at[xr, high], left_x),
    ]
    n_in = [
        ncopy(0, nbuf.at[xl, low], right_x),
        ncopy(1, nbuf.at[xr, high], left_x),
    ]
    for copy in n_out[:4]:
        copy.start()
    pump(3, 1)
    pump(3, 2)
    pump(4, 0)
    n_in[0].wait_recv()
    n_out[4].start()
    n_in[1].wait_recv()
    n_out[5].start()
    pump(4, 1)
    pump(4, 2)
    pump(5, 0)
    pump(5, 1)
    arrived(nbuf.at[0:2], n_r.at[2])
    normed = nbuf[...].reshape(NX * ROWS, D)

    def all_of(m):
        return remote(w.at[m], wp.at[m], wr_s, wr_r.at[m], partner)

    def hidden_of(buf):
        gate_part = jnp.dot(normed, buf[0].reshape(D, FFD), preferred_element_type=F32)
        lifted = jnp.dot(normed, buf[1].reshape(D, FFD), preferred_element_type=F32)
        return (gate_part / (1.0 + jnp.exp(-gate_part)) * lifted).astype(BF16)

    hidden = hidden_of(w)
    all_of(0).wait_recv()
    all_of(1).wait_recv()
    hidden_p = hidden_of(wp)
    pump(5, 2)
    all_of(2).wait_recv()
    def pcopy(n, src, dst, dev):
        return remote(src, dst, p_s, p_r.at[n], dev)

    def parts_of(cut):
        rows = (slice(None), slice(None), slice(None))
        pick = (2, slice(4 * cut, 4 * cut + 4)) + rows
        parts = lax.dot_general(hidden, w[pick].reshape(D // 2, FFD), NT, preferred_element_type=F32)
        parts = parts + lax.dot_general(
            hidden_p, wp[pick].reshape(D // 2, FFD), NT, preferred_element_type=F32
        )
        parts = parts.reshape(NX, ROWS, D // 2)
        psend[cut] = parts.astype(BF16)
        pown[cut] = parts

    def far_copy(cut, d):
        if d == 0:
            return pcopy(2 * cut, psend.at[cut, xf, low], pfar.at[cut, 0], right_x)
        return pcopy(2 * cut + 1, psend.at[cut, xf, high], pfar.at[cut, 1], left_x)

    def near_copies(cut):
        return [
            pcopy(4, psend.at[cut, xr, high], precv.at[cut, 0, high], right_x),
            pcopy(4, psend.at[cut, xl, low], precv.at[cut, 1, low], left_x),
        ]

    def mix(cut):
        far_copy(cut, 0).wait_recv()
        pmix[cut, 0] = (pown[cut, xr, low] + pfar[cut, 0].astype(F32)).astype(BF16)
        pcopy(4, pmix.at[cut, 0], precv.at[cut, 0, low], right_x).start()
        far_copy(cut, 1).wait_recv()
        pmix[cut, 1] = (pown[cut, xl, high] + pfar[cut, 1].astype(F32)).astype(BF16)
        pcopy(4, pmix.at[cut, 1], precv.at[cut, 1, high], left_x).start()

    for cut in range(2):
        parts_of(cut)
        far_copy(cut, 0).start()
        far_copy(cut, 1).start()
    for cut in range(2):
        for copy in near_copies(cut):
            copy.start()
    mix(0)
    mix(1)

    def drain():
        for h in range(2):
            sent(kv0.at[0, :, 0:7], ka_s.at[h])
            sent(kv0.at[0:7], kb_s.at[h])
        sent(w.at[:, z, 0:7], wa_s)
        sent(qbuf.at[0:3], q_s)
        sent(osend.at[0:7], o_s)
        sent(ow.at[0:7], ow_s)
        sent(nbuf.at[0:3], n_s)
        sent(w.at[:, 0:7], wb_s)
        sent(w, wr_s)

    def finish():
        for cut in range(2):
            columns = slice(cut * D // 2, (cut + 1) * D // 2)
            total = mid[:, columns].astype(F32) + pown[cut, x]
            total = total + precv[cut, 0].astype(F32) + precv[cut, 1].astype(F32)
            out_ref[:, columns] = total.astype(BF16)
        sent(psend.at[:, 0:3], p_s)

    drain()
    arrived(precv, p_r.at[4])
    finish()


def local(
    queries, keys, values, query_gain, key_gain, residual_in, out_weight, norm_gain,
    gate_weight, up_weight, down_weight,
):
    vmem = pl.BlockSpec(memory_space=pltpu.VMEM)
    dma = pltpu.SemaphoreType.DMA
    tables = [jnp.asarray(t) for t in rope_tables()]
    return pl.pallas_call(
        layer_kernel,
        name="layer",
        out_shape=jax.ShapeDtypeStruct((ROWS, D), BF16),
        in_specs=[pl.BlockSpec(memory_space=pl.ANY)] * 13,
        out_specs=vmem,
        scratch_shapes=[
            pltpu.VMEM((TOK, HEAD), BF16),
            pltpu.VMEM((KTOK, HEAD), BF16),
            pltpu.VMEM((1, HEAD), F32),
            pltpu.VMEM((1, HEAD), F32),
            pltpu.VMEM((ROWS, D), BF16),
            pltpu.VMEM((1, D), F32),
            pltpu.VMEM((2, 4, HEAD), F32),
            pltpu.VMEM((2, GRID_WIDTH, HEAD), F32),
            pltpu.VMEM((TEAM, TOK, HEAD), BF16),
            pltpu.VMEM((NZ, 2, NY, KH, HEAD), BF16),
            pltpu.VMEM((NY, 2, NZ, KH, HEAD), BF16),
            pltpu.VMEM((3, NZ, NY, 2, 16, FFD), BF16),
            pltpu.VMEM((3, NZ, NY, 2, 16, FFD), BF16),
            pltpu.VMEM((8, HEAD, D), BF16),
            pltpu.VMEM((TEAM, TOK, 2 * HEAD), F32),
            pltpu.VMEM((TEAM, TOK, HEAD), F32),
            pltpu.VMEM((8, ROWS, (TEAM + 1) * HEAD), BF16),
            pltpu.VMEM((8, ROWS, (TEAM + 1) * HEAD), BF16),
            pltpu.VMEM((ROWS, 8 * HEAD), BF16),
            pltpu.VMEM((NX, ROWS, D), BF16),
            pltpu.VMEM((ROWS, D), BF16),
            pltpu.VMEM((2, NX, ROWS, D // 2), BF16),
            pltpu.VMEM((2, NX, ROWS, D // 2), F32),
            pltpu.VMEM((2, 2, ROWS, D // 2), BF16),
            pltpu.VMEM((2, 2, 16, D // 2), BF16),
            pltpu.VMEM((2, 2, 16, D // 2), BF16),
            dma((11,)), dma, dma,
            dma((2,)), dma((2,)),
            dma, dma((4,)),
            dma((2,)), dma((4, 2)),
            dma, dma((4, 3)),
            dma, dma((3,)),
            dma, dma((5,)),
            dma, dma,
            dma, dma((3,)),
            dma, dma((5,)),
        ],
        compiler_params=pltpu.CompilerParams(
            collective_id=0, has_side_effects=True, vmem_limit_bytes=56 * 1024 * 1024
        ),
    )(
        queries, keys, values, query_gain.reshape(1, -1), key_gain.reshape(1, -1), residual_in,
        out_weight, norm_gain.reshape(1, -1),
        *[a.reshape(2, 16, FFD) for a in (gate_weight, up_weight, down_weight.T)], *tables,
    )


def solution(mesh):
    finer = Mesh(mesh.devices.reshape(NZ, NY, NX, 2), ("z", "y", "x", "c"))
    sp, tp = ("z", "y"), ("x", "c")
    in_specs = (
        P(sp, tp),
        P(sp, None),
        P(sp, None),
        P(),
        P(),
        P(sp + tp, None),
        P(tp, None),
        P(),
        P(sp, tp),
        P(sp, tp),
        P(tp, sp),
    )
    return jax.shard_map(
        local, mesh=finer, in_specs=in_specs, out_specs=P(sp + tp, None), check_vma=False
    )
```

```python
import math

import jax
import jax.numpy as jnp
import numpy as np
from jax import lax
from jax.experimental import pallas as pl
from jax.experimental.pallas import tpu as pltpu
from jax.sharding import Mesh
from jax.sharding import PartitionSpec as P

NZ = 8
NY = 8
RING = 8
NX = 4
HEAD = 128
GRID_WIDTH = 64
TOK = 256
TEAM = 4
KTOK = TOK // TEAM
KH = KTOK // 2
ROWS = 32
D = 2048
FFD = 384
EPS = 1e-06
ROPE_BASE = 10000.0
SCALE = HEAD ** (-0.5) * math.log2(math.e)
F32 = jnp.float32
BF16 = jnp.bfloat16
NT = (((1,), (1,)), ((), ()))
FAR_FIRST = (4, 1, 7, 3, 5, 2, 6)


def rope_tables():
    quarter = HEAD // 4
    inverse = ROPE_BASE ** (-np.arange(quarter, dtype=np.float64) * 2.0 / (HEAD // 2))
    rows = np.arange(NZ * NY * TOK // GRID_WIDTH, dtype=np.float64)[:, None] * inverse
    cols = np.arange(GRID_WIDTH, dtype=np.float64)[:, None] * inverse

    def half(angles):
        return (
            np.concatenate([np.cos(angles), np.cos(angles)], axis=1),
            np.concatenate([-np.sin(angles), np.sin(angles)], axis=1),
        )

    rc, rs = half(rows)
    cc, cs = half(cols)
    rc, rs = rc.reshape(-1, 4, HEAD // 2), rs.reshape(-1, 4, HEAD // 2)
    left = lambda a: np.concatenate([a, np.zeros_like(a)], axis=-1).astype(np.float32)
    right = lambda a: np.concatenate([np.zeros_like(a), a], axis=-1).astype(np.float32)
    return np.stack([left(rc), left(rs)], axis=1), np.stack([right(cc), right(cs)])


def normalize(x, gain):
    return x * lax.rsqrt(jnp.mean(x * x, axis=-1, keepdims=True) + EPS) * gain


def turn(x, cosine, sine):
    lane = lax.broadcasted_iota(jnp.int32, x.shape, 1)
    ahead = pltpu.roll(x, HEAD - 32, 1)
    behind = pltpu.roll(x, 32, 1)
    partner = jnp.where((lane // 32) % 2 == 0, ahead, behind)
    return x * cosine + partner * sine


def layer_kernel(
    q_hbm, k_hbm, v_hbm, qg_hbm, kg_hbm, res_hbm, ow_hbm, ng_hbm, gate_hbm, up_hbm, down_hbm,
    row_hbm, col_hbm,
    out_ref,
    q_ref, k_ref, qg_ref, kg_ref, res_ref, ng_ref, row_ref, col_ref,
    qbuf, kv0, kv1, w, wp, ow, acc, peak, osend, orecv, att, nbuf, mid, psend, pown, precv, pfar, pmix,
    in_s, q_s, q_r, ka_s, ka_r, wa_s, wa_r, wo_s, wo_r, kb_s, kb_r, wb_s, wb_r, wr_s, wr_r, wro_r,
    ow_s, ow_r, o_s, o_r, n_s, n_r, p_s, p_r,
):
    z = lax.axis_index("z")
    y = lax.axis_index("y")
    x = lax.axis_index("x")
    c = lax.axis_index("c")
    tp = x * 2 + c
    team = x // 2
    j = lax.rem(x, 2) * 2 + c
    s = z * NY + y
    pos = (z, y)
    axis = ("z", "y")

    def wrap(v, n=RING):
        return lax.rem(v + n, n)

    def tp_id(i):
        return {"x": i // 2, "c": lax.rem(i, 2)}

    barrier = pltpu.get_barrier_semaphore()

    def greet(d, carry):
        pl.semaphore_signal(barrier, inc=1, device_id={"z": wrap(z + d)})
        pl.semaphore_signal(barrier, inc=1, device_id={"y": wrap(y + d)})
        pl.semaphore_signal(barrier, inc=1, device_id=tp_id(wrap(tp + d)))
        return carry

    lax.fori_loop(1, RING, greet, 0)

    lanes = pl.ds(pl.multiple_of(team * HEAD, HEAD), HEAD)

    def key_rows(half):
        return pl.ds(pl.multiple_of(j * KTOK + half * KH, KH), KH)

    loads = [
        (k_hbm.at[pl.ds(pl.multiple_of(j * KTOK, KTOK), KTOK), lanes], k_ref),
        (row_hbm.at[s], row_ref),
        (col_hbm, col_ref),
        (kg_hbm, kg_ref),
        (q_hbm, q_ref),
        (qg_hbm, qg_ref),
        (ow_hbm, ow.at[tp]),
        (res_hbm, res_ref),
        (ng_hbm, ng_ref),
        (v_hbm.at[key_rows(0), lanes], kv0.at[z, 1, y]),
        (v_hbm.at[key_rows(1), lanes], kv1.at[y, 1, z]),
        (gate_hbm.at[0], w.at[0, 0, z, 0]),
        (gate_hbm.at[1], w.at[1, 0, y, 0]),
        (up_hbm.at[0], w.at[0, 1, z, 0]),
        (up_hbm.at[1], w.at[1, 1, y, 0]),
        (down_hbm.at[0], w.at[0, 2, z, 0]),
        (down_hbm.at[1], w.at[1, 2, y, 0]),
    ]
    sems = [in_s.at[n] for n in (0, 1, 2, 3, 4, 5, 6, 7, 8, 9, 9, 10, 10, 10, 10, 10, 10)]
    loads = [pltpu.make_async_copy(a, b, m) for (a, b), m in zip(loads, sems)]

    def landed(ref, sem):
        pltpu.make_async_copy(ref, ref, sem).wait()

    for load in loads:
        load.start()

    for load in loads[:4]:
        load.wait()
    cosine = row_ref[0, pl.ds(j, 1), :] + col_ref[0]
    sine = row_ref[1, pl.ds(j, 1), :] + col_ref[1]
    kk = k_ref[...].astype(F32)
    kk = turn(normalize(kk, kg_ref[...]), cosine, sine).astype(BF16)
    kv0[z, 0, y] = kk[:KH]
    kv1[y, 0, z] = kk[KH:]
    landed(kv0.at[z, 1, 0:2], in_s.at[9])
    pl.semaphore_wait(barrier, 21)

    partner = {"c": 1 - c}

    def remote(ref, dst, ss, rs, dev):
        return pltpu.make_async_remote_copy(
            src_ref=ref, dst_ref=dst, send_sem=ss, recv_sem=rs,
            device_id=dev, device_id_type=pl.DeviceIdType.MESH,
        )

    def arrived(ref, sem):
        remote(ref, ref, sem, sem, partner).wait_recv()

    def sent(ref, sem):
        remote(ref, ref, sem, sem, partner).wait_send()

    def kva(h, d):
        ref = kv0.at[z, :, y] if h == 0 else kv1.at[y, :, z]
        dev = {"y": wrap(y + d)} if h == 0 else {"z": wrap(z + d)}
        return remote(ref, ref, ka_s.at[h], ka_r.at[min(d, RING - d) - 1], dev)

    def wa(h, d, k):
        src, dst = ((1 - k) % RING, -k % RING) if d == 0 else (k - 1, k)
        pick = slice(0, 3) if k < 4 else (slice(0, 2) if d == 0 else slice(2, 3))
        step = 1 if d == 0 else -1
        dev = {"y": wrap(y + step)} if h == 0 else {"z": wrap(z + step)}
        return remote(
            w.at[h, pick, pos[h], src], w.at[h, pick, pos[h], dst], wa_s, wa_r.at[k - 1], dev
        )

    def four(k):
        return w.at[0, :, 0 : 4 if k < 5 else 2, 0]

    def w_first(k):
        if k > 1:
            arrived(four(k), wa_r.at[k - 2])
        if k <= 4:
            for h in range(2):
                for d in range(2):
                    wa(h, d, k).start()

    def own_ref(buf, h, d, k, shift):
        pick = slice(0, 3) if k < 4 else (slice(0, 2) if d == 0 else slice(2, 3))
        return buf.at[h, pick, wrap(pos[h] + shift * (-1 if d == 0 else 1)), 0]

    def own_pass(k):
        if k > 1:
            arrived(four(k), wo_r.at[k - 2])
        for h in range(2):
            for d in range(2):
                if k <= 4:
                    ref = own_ref(w, h, d, k, k - 1)
                    dev = {axis[h]: wrap(pos[h] + (1 if d == 0 else -1))}
                    remote(ref, ref, wo_s, wo_r.at[k - 1], dev).start()
        for h in range(2):
            for d in range(2):
                if k > 1:
                    src, dst = own_ref(w, h, d, k - 1, k - 1), own_ref(wp, h, d, k - 1, k - 1)
                    remote(src, dst, wr_s, wro_r, partner).start()
                elif d == 0:
                    src, dst = own_ref(w, h, d, 1, 0), own_ref(wp, h, d, 1, 0)
                    remote(src, dst, wr_s, wro_r, partner).start()

    def kv_piece(h, e):
        ref = kv0.at[z, :, wrap(y + e)] if h == 0 else kv1.at[y, :, wrap(z + e)]
        for d in range(2):
            dev = {axis[h]: wrap(pos[h] + (1 if d == 0 else -1))}
            remote(ref, ref, kb_s.at[h], kb_r.at[0, 0], dev).start()

    def kv_group(g):
        if g > 0:
            arrived(kv0.at[0, :, 0 : 4 if g < 4 else 2], ka_r.at[g - 1])
        for h in range(2):
            for e in sorted({g % RING, -g % RING}):
                kv_piece(h, e)

    def start_kva(d):
        kva(0, d).start()
        kva(1, d).start()

    kv_group(0)
    landed(w.at[:, :, 0, 0], in_s.at[10])
    w_first(1)
    for d in FAR_FIRST:
        start_kva(d)
    own_pass(1)

    loads[4].wait()
    loads[5].wait()
    for r in range(4):
        part = slice(r * GRID_WIDTH, (r + 1) * GRID_WIDTH)
        cosine = row_ref[0, r : r + 1, :] + col_ref[0]
        sine = row_ref[1, r : r + 1, :] + col_ref[1]
        qq = turn(normalize(q_ref[part, :].astype(F32), qg_ref[...]), cosine, sine)
        qbuf[j, part] = (qq * SCALE).astype(BF16)
    peak[...] = jnp.full(peak.shape, -1e30, F32)
    acc[...] = jnp.zeros(acc.shape, F32)

    def qcopy(d):
        other = team * TEAM + lax.rem(j + d, TEAM)
        return remote(qbuf.at[j], qbuf.at[j], q_s, q_r, tp_id(other))

    for d in range(1, TEAM):
        qcopy(d).start()

    right_x = {"x": wrap(x + 1, NX)}
    left_x = {"x": wrap(x - 1, NX)}
    tl = wrap(x - 1, NX) * 2 + c
    tr = wrap(x + 1, NX) * 2 + c
    far = wrap(x + 2, NX) * 2 + c

    def head_ref(i, part=None):
        if part is None:
            return ow.at[i]
        return ow.at[i, pl.ds(part * 64, 64)]

    def owcopy(n, ref, dev):
        return remote(ref, ref, ow_s, ow_r.at[n], dev)

    ow_out = [
        owcopy(0, head_ref(tp), right_x),
        owcopy(1, head_ref(tp), left_x),
        owcopy(4, head_ref(tp), partner),
        owcopy(2, head_ref(tl, 0), right_x),
        owcopy(3, head_ref(tr, 1), left_x),
        owcopy(4, head_ref(tl), partner),
        owcopy(4, head_ref(tr), partner),
        owcopy(4, head_ref(far, 0), partner),
        owcopy(4, head_ref(far, 1), partner),
    ]
    ow_in = [
        owcopy(0, head_ref(tl), right_x),
        owcopy(1, head_ref(tr), left_x),
        owcopy(2, head_ref(far, 0), right_x),
        owcopy(3, head_ref(far, 1), left_x),
    ]
    loads[6].wait()

    for n in range(3):
        ow_out[n].start()

    def kvb(h, d, k, q):
        shift = (k - 1) * (-1 if d == 0 else 1)
        buf = kv0 if h == 0 else kv1
        ref = buf.at[wrap(pos[h] + shift), q // 2, pl.ds(4 * (q % 2), 4)]
        dev = {axis[h]: wrap(pos[h] + (1 if d == 0 else -1))}
        return remote(ref, ref, kb_s.at[h], kb_r.at[k - 1, q], dev)

    def kv_pass(k):
        if k == 2:
            arrived(kv0.at[0:4], kb_r.at[0, 0])
        for q in range(4):
            if k > 2:
                arrived(kv0.at[0, 0 : 2 if k < 5 else 1], kb_r.at[k - 2, q])
            if k <= 4:
                for h in range(2):
                    for d in range(2):
                        if k < 4 or d == q // 2:
                            kvb(h, d, k, q).start()

    def rest(buf, h, d, k, m, shift):
        lo, hi = (1, RING) if k < 4 else ((1, 5) if d == 0 else (5, RING))
        return buf.at[h, m, wrap(pos[h] + shift * (-1 if d == 0 else 1)), lo:hi]

    def pump(k, m):
        if k > 1:
            arrived(w.at[0, m, 0 : 4 if k < 5 else 2, 1:RING], wb_r.at[k - 2, m])
        for h in range(2):
            for d in range(2):
                if k <= 4:
                    ref = rest(w, h, d, k, m, k - 1)
                    dev = {axis[h]: wrap(pos[h] + (1 if d == 0 else -1))}
                    remote(ref, ref, wb_s, wb_r.at[k - 1, m], dev).start()
        for h in range(2):
            for d in range(2):
                if k > 1:
                    src, dst = rest(w, h, d, k - 1, m, k - 1), rest(wp, h, d, k - 1, m, k - 1)
                    remote(src, dst, wr_s, wr_r.at[m], partner).start()
                elif d == 0:
                    src, dst = rest(w, h, d, 1, m, 0), rest(wp, h, d, 1, m, 0)
                    remote(src, dst, wr_s, wr_r.at[m], partner).start()

    ones = jnp.ones((1, HEAD), BF16)

    def attend(blocks):
        keys = jnp.concatenate([buf[b, 0].reshape(256, HEAD) for buf, b in blocks], axis=0)
        vals = jnp.concatenate([buf[b, 1].reshape(256, HEAD) for buf, b in blocks], axis=0)
        wide = keys.shape[0]
        vals = jnp.concatenate([vals, jnp.broadcast_to(ones, vals.shape)], axis=1)

        def scores_of(h):
            return lax.dot_general(qbuf[h], keys, NT, preferred_element_type=F32)

        scores = scores_of(0)
        for h in range(TEAM):
            later = scores_of(h + 1) if h + 1 < TEAM else None
            old = peak[h]
            new = jnp.maximum(old, jnp.max(scores, axis=1, keepdims=True))
            factor = jnp.exp2(old - new)
            peak[h] = new
            raw = jnp.exp2(scores - jnp.concatenate([new] * (wide // HEAD), axis=1)).astype(BF16)
            update = jnp.dot(raw, vals, preferred_element_type=F32)
            acc[h] = acc[h] * jnp.concatenate([factor, factor], axis=1) + update
            scores = later

    w_first(2)
    kv_group(1)
    kv_group(2)
    kv_group(3)
    kv_group(4)
    w_first(3)
    own_pass(2)
    arrived(qbuf.at[0:3], q_r)
    attend([(kv0, z), (kv1, y)])
    kv_pass(2)
    w_first(4)
    own_pass(3)
    attend([(kv0, wrap(z - 1)), (kv0, wrap(z + 1)), (kv1, wrap(y - 1)), (kv1, wrap(y + 1))])
    kv_pass(3)
    w_first(5)
    own_pass(4)
    pump(1, 0)
    ow_in[0].wait_recv()
    ow_out[3].start()
    ow_in[1].wait_recv()
    ow_out[4].start()
    ow_out[5].start()
    ow_out[6].start()
    attend([(kv0, wrap(z - 2)), (kv0, wrap(z + 2)), (kv1, wrap(y - 2)), (kv1, wrap(y + 2))])
    kv_pass(4)
    pump(1, 1)
    pump(1, 2)
    attend([(kv0, wrap(z - 3)), (kv0, wrap(z + 3)), (kv1, wrap(y - 3)), (kv1, wrap(y + 3))])
    own_pass(5)
    kv_pass(5)
    attend([(kv0, wrap(z + 4)), (kv1, wrap(y + 4))])
    pump(2, 0)
    pump(2, 1)

    lane = lax.broadcasted_iota(jnp.int32, (TOK, HEAD), 1)
    tops = jnp.zeros((TOK, HEAD), F32)
    sums = jnp.ones((TOK, HEAD), F32)
    for h in range(TEAM):
        total = acc[h, :, HEAD:]
        mean = (acc[h, :, :HEAD] / total).astype(BF16)
        osend[:, :, h * HEAD : (h + 1) * HEAD] = mean.reshape(8, ROWS, HEAD)
        tops = jnp.where(lane == h, peak[h], tops)
        sums = jnp.where(lane == h, total, sums)
    level = tops + jnp.log2(sums)
    first = level.astype(BF16).astype(F32)
    second = (level - first).astype(BF16).astype(F32)
    third = level - first - second
    stats = first + pltpu.roll(second, 4, 1) + pltpu.roll(third, 8, 1)
    osend[:, :, TEAM * HEAD :] = stats.astype(BF16).reshape(8, ROWS, HEAD)

    def ocopy(d):
        i = wrap(tp + d)
        return remote(osend.at[i], orecv.at[tp], o_s, o_r, tp_id(i))

    for d in (4, 3, 5, 2, 6, 1, 7):
        ocopy(d).start()
    orecv[tp] = osend[tp]

    pump(2, 2)
    ow_in[2].wait_recv()
    ow_out[7].start()
    ow_in[3].wait_recv()
    ow_out[8].start()
    pump(3, 0)

    arrived(orecv.at[0:7], o_r)
    for t in range(2):
        levels = []
        for i in range(t * TEAM, (t + 1) * TEAM):
            st = orecv[i, :, TEAM * HEAD :].astype(F32)
            levels.append(st + pltpu.roll(st, HEAD - 4, 1) + pltpu.roll(st, HEAD - 8, 1))
        top = jnp.maximum(jnp.maximum(levels[0], levels[1]), jnp.maximum(levels[2], levels[3]))
        shares = [jnp.exp2(v - top) for v in levels]
        total = shares[0] + shares[1] + shares[2] + shares[3]
        shares = [v / total for v in shares]
        for h in range(TEAM):
            mixed = jnp.zeros((ROWS, HEAD), F32)
            for i in range(TEAM):
                block = orecv[t * TEAM + i, :, h * HEAD : (h + 1) * HEAD].astype(F32)
                mixed = mixed + block * shares[i][:, h : h + 1]
            at = (t * TEAM + h) * HEAD
            att[:, at : at + HEAD] = mixed.astype(BF16)

    arrived(ow.at[0:4], ow_r.at[4])
    loads[7].wait()
    loads[8].wait()
    projected = jnp.dot(att[...], ow[...].reshape(8 * HEAD, D), preferred_element_type=F32)
    middle = (res_ref[...].astype(F32) + projected).astype(BF16)
    mid[...] = middle
    nbuf[x] = normalize(middle.astype(F32), ng_ref[...]).astype(BF16)

    def ncopy(n, ref, dev):
        return remote(ref, ref, n_s, n_r.at[min(n, 2)], dev)

    xl, xr, xf = wrap(x - 1, NX), wrap(x + 1, NX), wrap(x + 2, NX)
    low, high = pl.ds(0, 16), pl.ds(16, 16)
    n_out = [
        ncopy(0, nbuf.at[x, low], right_x),
        ncopy(1, nbuf.at[x, high], left_x),
        ncopy(2, nbuf.at[x, high], right_x),
        ncopy(3, nbuf.at[x, low], left_x),
        ncopy(4, nbuf.at[xl, low], right_x),
        ncopy(5, nbuf.at[xr, high], left_x),
    ]
    n_in = [
        ncopy(0, nbuf.at[xl, low], right_x),
        ncopy(1, nbuf.at[xr, high], left_x),
    ]
    for copy in n_out[:4]:
        copy.start()
    pump(3, 1)
    pump(3, 2)
    pump(4, 0)
    n_in[0].wait_recv()
    n_out[4].start()
    n_in[1].wait_recv()
    n_out[5].start()
    pump(4, 1)
    pump(4, 2)
    pump(5, 0)
    pump(5, 1)
    arrived(nbuf.at[0:2], n_r.at[2])
    normed = nbuf[...].reshape(NX * ROWS, D)

    def all_of(m):
        return remote(w.at[:, m, :, 1:RING], wp.at[:, m, :, 1:RING], wr_s, wr_r.at[m], partner)

    back_y = [wrap(i - y) for i in range(RING)]
    back_z = [wrap(i - z) for i in range(RING)]

    def matrix(buf, m, places=range(NZ)):
        blocks = []
        for i in places:
            for k in range(NY):
                blocks += [buf[0, m, i, back_y[k]], buf[1, m, k, back_z[i]]]
        return jnp.concatenate(blocks, axis=0)

    def hidden_of(buf):
        gate_part = jnp.dot(normed, matrix(buf, 0), preferred_element_type=F32)
        lifted = jnp.dot(normed, matrix(buf, 1), preferred_element_type=F32)
        return (gate_part / (1.0 + jnp.exp(-gate_part)) * lifted).astype(BF16)

    hidden = hidden_of(w)
    arrived(w.at[:, :, :, 0], wro_r)
    all_of(0).wait_recv()
    all_of(1).wait_recv()
    hidden_p = hidden_of(wp)
    pump(5, 2)
    def pcopy(n, src, dst, dev):
        return remote(src, dst, p_s, p_r.at[n], dev)

    def parts_of(left, buf, cut):
        places = range(4 * cut, 4 * cut + 4)
        parts = lax.dot_general(left, matrix(buf, 2, places), NT, preferred_element_type=F32)
        return parts.reshape(NX, ROWS, D // 2)

    def far_copy(cut, d):
        if d == 0:
            return pcopy(2 * cut, psend.at[cut, xf, low], pfar.at[cut, 0], right_x)
        return pcopy(2 * cut + 1, psend.at[cut, xf, high], pfar.at[cut, 1], left_x)

    def near_copies(cut):
        return [
            pcopy(4, psend.at[cut, xr, high], precv.at[cut, 0, high], right_x),
            pcopy(4, psend.at[cut, xl, low], precv.at[cut, 1, low], left_x),
        ]

    def mix(cut):
        far_copy(cut, 0).wait_recv()
        pmix[cut, 0] = (pown[cut, xr, low] + pfar[cut, 0].astype(F32)).astype(BF16)
        pcopy(4, pmix.at[cut, 0], precv.at[cut, 0, low], right_x).start()
        far_copy(cut, 1).wait_recv()
        pmix[cut, 1] = (pown[cut, xl, high] + pfar[cut, 1].astype(F32)).astype(BF16)
        pcopy(4, pmix.at[cut, 1], precv.at[cut, 1, high], left_x).start()

    for cut in range(2):
        pown[cut] = parts_of(hidden, w, cut)
    all_of(2).wait_recv()
    for cut in range(2):
        parts = pown[cut] + parts_of(hidden_p, wp, cut)
        pown[cut] = parts
        psend[cut] = parts.astype(BF16)
        far_copy(cut, 0).start()
        far_copy(cut, 1).start()
    for cut in range(2):
        for copy in near_copies(cut):
            copy.start()
    mix(0)
    mix(1)

    def drain():
        for h in range(2):
            sent(kv0.at[0, :, 0:7], ka_s.at[h])
            sent(kv0.at[0:7], kb_s.at[h])
        sent(w.at[:, :, 0:7, 0], wa_s)
        sent(w.at[:, :, 0:7, 0], wo_s)
        sent(qbuf.at[0:3], q_s)
        sent(osend.at[0:7], o_s)
        sent(ow.at[0:7], ow_s)
        sent(nbuf.at[0:3], n_s)
        sent(w.at[:, :, 0:7, 1:RING], wb_s)
        sent(w, wr_s)

    def finish():
        for cut in range(2):
            columns = slice(cut * D // 2, (cut + 1) * D // 2)
            total = mid[:, columns].astype(F32) + pown[cut, x]
            total = total + precv[cut, 0].astype(F32) + precv[cut, 1].astype(F32)
            out_ref[:, columns] = total.astype(BF16)
        sent(psend.at[:, 0:3], p_s)

    drain()
    arrived(precv, p_r.at[4])
    finish()


def local(
    queries, keys, values, query_gain, key_gain, residual_in, out_weight, norm_gain,
    gate_weight, up_weight, down_weight,
):
    vmem = pl.BlockSpec(memory_space=pltpu.VMEM)
    dma = pltpu.SemaphoreType.DMA
    tables = [jnp.asarray(t) for t in rope_tables()]
    return pl.pallas_call(
        layer_kernel,
        name="layer",
        out_shape=jax.ShapeDtypeStruct((ROWS, D), BF16),
        in_specs=[pl.BlockSpec(memory_space=pl.ANY)] * 13,
        out_specs=vmem,
        scratch_shapes=[
            pltpu.VMEM((TOK, HEAD), BF16),
            pltpu.VMEM((KTOK, HEAD), BF16),
            pltpu.VMEM((1, HEAD), F32),
            pltpu.VMEM((1, HEAD), F32),
            pltpu.VMEM((ROWS, D), BF16),
            pltpu.VMEM((1, D), F32),
            pltpu.VMEM((2, 4, HEAD), F32),
            pltpu.VMEM((2, GRID_WIDTH, HEAD), F32),
            pltpu.VMEM((TEAM, TOK, HEAD), BF16),
            pltpu.VMEM((NZ, 2, NY, KH, HEAD), BF16),
            pltpu.VMEM((NY, 2, NZ, KH, HEAD), BF16),
            pltpu.VMEM((2, 3, RING, RING, 16, FFD), BF16),
            pltpu.VMEM((2, 3, RING, RING, 16, FFD), BF16),
            pltpu.VMEM((8, HEAD, D), BF16),
            pltpu.VMEM((TEAM, TOK, 2 * HEAD), F32),
            pltpu.VMEM((TEAM, TOK, HEAD), F32),
            pltpu.VMEM((8, ROWS, (TEAM + 1) * HEAD), BF16),
            pltpu.VMEM((8, ROWS, (TEAM + 1) * HEAD), BF16),
            pltpu.VMEM((ROWS, 8 * HEAD), BF16),
            pltpu.VMEM((NX, ROWS, D), BF16),
            pltpu.VMEM((ROWS, D), BF16),
            pltpu.VMEM((2, NX, ROWS, D // 2), BF16),
            pltpu.VMEM((2, NX, ROWS, D // 2), F32),
            pltpu.VMEM((2, 2, ROWS, D // 2), BF16),
            pltpu.VMEM((2, 2, 16, D // 2), BF16),
            pltpu.VMEM((2, 2, 16, D // 2), BF16),
            dma((11,)), dma, dma,
            dma((2,)), dma((4,)),
            dma, dma((4,)),
            dma, dma((4,)),
            dma((2,)), dma((4, 4)),
            dma, dma((4, 3)),
            dma, dma((3,)), dma,
            dma, dma((5,)),
            dma, dma,
            dma, dma((3,)),
            dma, dma((5,)),
        ],
        compiler_params=pltpu.CompilerParams(
            collective_id=0, has_side_effects=True, vmem_limit_bytes=56 * 1024 * 1024
        ),
    )(
        queries, keys, values, query_gain.reshape(1, -1), key_gain.reshape(1, -1), residual_in,
        out_weight, norm_gain.reshape(1, -1),
        *[a.reshape(2, 16, FFD) for a in (gate_weight, up_weight, down_weight.T)], *tables,
    )


def solution(mesh):
    finer = Mesh(mesh.devices.reshape(NZ, NY, NX, 2), ("z", "y", "x", "c"))
    sp, tp = ("z", "y"), ("x", "c")
    in_specs = (
        P(sp, tp),
        P(sp, None),
        P(sp, None),
        P(),
        P(),
        P(sp + tp, None),
        P(tp, None),
        P(),
        P(sp, tp),
        P(sp, tp),
        P(tp, sp),
    )
    return jax.shard_map(
        local, mesh=finer, in_specs=in_specs, out_specs=P(sp + tp, None), check_vma=False
    )
```

```python
import math

import jax
import jax.numpy as jnp
import numpy as np
from jax import lax
from jax.experimental import pallas as pl
from jax.experimental.pallas import tpu as pltpu
from jax.sharding import Mesh
from jax.sharding import PartitionSpec as P

NZ = 8
NY = 8
RING = 8
NX = 4
HEAD = 128
GRID_WIDTH = 64
TOK = 256
TEAM = 4
KTOK = TOK // TEAM
KH = KTOK // 2
ROWS = 32
D = 2048
FFD = 384
EPS = 1e-06
ROPE_BASE = 10000.0
SCALE = HEAD ** (-0.5) * math.log2(math.e)
F32 = jnp.float32
BF16 = jnp.bfloat16
NT = (((1,), (1,)), ((), ()))
FAR_FIRST = (4, 1, 7, 3, 5, 2, 6)


def rope_tables():
    quarter = HEAD // 4
    inverse = ROPE_BASE ** (-np.arange(quarter, dtype=np.float64) * 2.0 / (HEAD // 2))
    rows = np.arange(NZ * NY * TOK // GRID_WIDTH, dtype=np.float64)[:, None] * inverse
    cols = np.arange(GRID_WIDTH, dtype=np.float64)[:, None] * inverse

    def half(angles):
        return (
            np.concatenate([np.cos(angles), np.cos(angles)], axis=1),
            np.concatenate([-np.sin(angles), np.sin(angles)], axis=1),
        )

    rc, rs = half(rows)
    cc, cs = half(cols)
    rc, rs = rc.reshape(-1, 4, HEAD // 2), rs.reshape(-1, 4, HEAD // 2)
    left = lambda a: np.concatenate([a, np.zeros_like(a)], axis=-1).astype(np.float32)
    right = lambda a: np.concatenate([np.zeros_like(a), a], axis=-1).astype(np.float32)
    return np.stack([left(rc), left(rs)], axis=1), np.stack([right(cc), right(cs)])


def normalize(x, gain):
    return x * lax.rsqrt(jnp.mean(x * x, axis=-1, keepdims=True) + EPS) * gain


def turn(x, cosine, sine):
    lane = lax.broadcasted_iota(jnp.int32, x.shape, 1)
    ahead = pltpu.roll(x, HEAD - 32, 1)
    behind = pltpu.roll(x, 32, 1)
    partner = jnp.where((lane // 32) % 2 == 0, ahead, behind)
    return x * cosine + partner * sine


def layer_kernel(
    q_hbm, k_hbm, v_hbm, qg_hbm, kg_hbm, res_hbm, ow_hbm, ng_hbm, gate_hbm, up_hbm, down_hbm,
    row_hbm, col_hbm,
    out_ref,
    q_ref, k_ref, qg_ref, kg_ref, res_ref, ng_ref, row_ref, col_ref,
    qbuf, kv0, kv1, w, wp, ow, acc, peak, osend, orecv, att, nbuf, mid, psend, pown, precv, pfar, pmix,
    in_s, q_s, q_r, ka_s, ka_r, wa_s, wa_r, wo_s, wo_r, kb_s, kb_r, wb_s, wb_r, wr_s, wr_r, wro_r,
    ow_s, ow_r, o_s, o_r, n_s, n_r, p_s, p_r,
):
    z = lax.axis_index("z")
    y = lax.axis_index("y")
    x = lax.axis_index("x")
    c = lax.axis_index("c")
    tp = x * 2 + c
    team = x // 2
    j = lax.rem(x, 2) * 2 + c
    s = z * NY + y
    pos = (z, y)
    axis = ("z", "y")

    def wrap(v, n=RING):
        return lax.rem(v + n, n)

    def tp_id(i):
        return {"x": i // 2, "c": lax.rem(i, 2)}

    barrier = pltpu.get_barrier_semaphore()

    def greet(d, carry):
        pl.semaphore_signal(barrier, inc=1, device_id={"z": wrap(z + d)})
        pl.semaphore_signal(barrier, inc=1, device_id={"y": wrap(y + d)})
        pl.semaphore_signal(barrier, inc=1, device_id=tp_id(wrap(tp + d)))
        return carry

    lax.fori_loop(1, RING, greet, 0)

    lanes = pl.ds(pl.multiple_of(team * HEAD, HEAD), HEAD)

    def key_rows(half):
        return pl.ds(pl.multiple_of(j * KTOK + half * KH, KH), KH)

    loads = [
        (k_hbm.at[pl.ds(pl.multiple_of(j * KTOK, KTOK), KTOK), lanes], k_ref),
        (row_hbm.at[s], row_ref),
        (col_hbm, col_ref),
        (kg_hbm, kg_ref),
        (q_hbm, q_ref),
        (qg_hbm, qg_ref),
        (ow_hbm, ow.at[tp]),
        (res_hbm, res_ref),
        (ng_hbm, ng_ref),
        (v_hbm.at[key_rows(0), lanes], kv0.at[z, 1, y]),
        (v_hbm.at[key_rows(1), lanes], kv1.at[y, 1, z]),
        (gate_hbm.at[0], w.at[0, 0, z, 0]),
        (gate_hbm.at[1], w.at[1, 0, y, 0]),
        (up_hbm.at[0], w.at[0, 1, z, 0]),
        (up_hbm.at[1], w.at[1, 1, y, 0]),
        (down_hbm.at[0], w.at[0, 2, z, 0]),
        (down_hbm.at[1], w.at[1, 2, y, 0]),
    ]
    sems = [in_s.at[n] for n in (0, 1, 2, 3, 4, 5, 6, 7, 8, 9, 9, 10, 10, 10, 10, 10, 10)]
    loads = [pltpu.make_async_copy(a, b, m) for (a, b), m in zip(loads, sems)]

    def landed(ref, sem):
        pltpu.make_async_copy(ref, ref, sem).wait()

    for load in loads:
        load.start()

    for load in loads[:4]:
        load.wait()
    cosine = row_ref[0, pl.ds(j, 1), :] + col_ref[0]
    sine = row_ref[1, pl.ds(j, 1), :] + col_ref[1]
    kk = k_ref[...].astype(F32)
    kk = turn(normalize(kk, kg_ref[...]), cosine, sine).astype(BF16)
    kv0[z, 0, y] = kk[:KH]
    kv1[y, 0, z] = kk[KH:]
    landed(kv0.at[z, 1, 0:2], in_s.at[9])
    pl.semaphore_wait(barrier, 21)

    partner = {"c": 1 - c}

    def remote(ref, dst, ss, rs, dev):
        return pltpu.make_async_remote_copy(
            src_ref=ref, dst_ref=dst, send_sem=ss, recv_sem=rs,
            device_id=dev, device_id_type=pl.DeviceIdType.MESH,
        )

    def arrived(ref, sem):
        remote(ref, ref, sem, sem, partner).wait_recv()

    def sent(ref, sem):
        remote(ref, ref, sem, sem, partner).wait_send()

    def kva(h, d):
        ref = kv0.at[z, :, y] if h == 0 else kv1.at[y, :, z]
        dev = {"y": wrap(y + d)} if h == 0 else {"z": wrap(z + d)}
        return remote(ref, ref, ka_s.at[h], ka_r.at[min(d, RING - d) - 1], dev)

    def wa(h, d, k):
        src, dst = ((1 - k) % RING, -k % RING) if d == 0 else (k - 1, k)
        pick = slice(0, 3) if k < 4 else (slice(0, 2) if d == 0 else slice(2, 3))
        step = 1 if d == 0 else -1
        dev = {"y": wrap(y + step)} if h == 0 else {"z": wrap(z + step)}
        return remote(
            w.at[h, pick, pos[h], src], w.at[h, pick, pos[h], dst], wa_s, wa_r.at[k - 1], dev
        )

    def four(k):
        return w.at[0, :, 0 : 4 if k < 5 else 2, 0]

    def w_first(k):
        if k > 1:
            arrived(four(k), wa_r.at[k - 2])
        if k <= 4:
            for h in range(2):
                for d in range(2):
                    wa(h, d, k).start()

    def own_ref(buf, h, d, k, shift):
        pick = slice(0, 3) if k < 4 else (slice(0, 2) if d == 0 else slice(2, 3))
        return buf.at[h, pick, wrap(pos[h] + shift * (-1 if d == 0 else 1)), 0]

    def own_pass(k):
        if k > 1:
            arrived(four(k), wo_r.at[k - 2])
        for h in range(2):
            for d in range(2):
                if k <= 4:
                    ref = own_ref(w, h, d, k, k - 1)
                    dev = {axis[h]: wrap(pos[h] + (1 if d == 0 else -1))}
                    remote(ref, ref, wo_s, wo_r.at[k - 1], dev).start()
        for h in range(2):
            for d in range(2):
                if k > 1:
                    src, dst = own_ref(w, h, d, k - 1, k - 1), own_ref(wp, h, d, k - 1, k - 1)
                    remote(src, dst, wr_s, wro_r, partner).start()
                elif d == 0:
                    src, dst = own_ref(w, h, d, 1, 0), own_ref(wp, h, d, 1, 0)
                    remote(src, dst, wr_s, wro_r, partner).start()

    def kv_piece(h, e):
        ref = kv0.at[z, :, wrap(y + e)] if h == 0 else kv1.at[y, :, wrap(z + e)]
        for d in range(2):
            dev = {axis[h]: wrap(pos[h] + (1 if d == 0 else -1))}
            remote(ref, ref, kb_s.at[h], kb_r.at[0, 0], dev).start()

    def kv_group(g):
        if g > 0:
            arrived(kv0.at[0, :, 0 : 4 if g < 4 else 2], ka_r.at[g - 1])
        for h in range(2):
            for e in sorted({g % RING, -g % RING}):
                kv_piece(h, e)

    def start_kva(d):
        kva(0, d).start()
        kva(1, d).start()

    kv_group(0)
    landed(w.at[:, :, 0, 0], in_s.at[10])
    w_first(1)
    for d in FAR_FIRST:
        start_kva(d)
    own_pass(1)

    loads[4].wait()
    loads[5].wait()
    for r in range(4):
        part = slice(r * GRID_WIDTH, (r + 1) * GRID_WIDTH)
        cosine = row_ref[0, r : r + 1, :] + col_ref[0]
        sine = row_ref[1, r : r + 1, :] + col_ref[1]
        qq = turn(normalize(q_ref[part, :].astype(F32), qg_ref[...]), cosine, sine)
        qbuf[j, part] = (qq * SCALE).astype(BF16)
    peak[...] = jnp.full(peak.shape, -1e30, F32)
    acc[...] = jnp.zeros(acc.shape, F32)

    def qcopy(d):
        other = team * TEAM + lax.rem(j + d, TEAM)
        return remote(qbuf.at[j], qbuf.at[j], q_s, q_r, tp_id(other))

    for d in range(1, TEAM):
        qcopy(d).start()

    right_x = {"x": wrap(x + 1, NX)}
    left_x = {"x": wrap(x - 1, NX)}
    tl = wrap(x - 1, NX) * 2 + c
    tr = wrap(x + 1, NX) * 2 + c
    far = wrap(x + 2, NX) * 2 + c

    def head_ref(i, part=None):
        if part is None:
            return ow.at[i]
        return ow.at[i, pl.ds(part * 64, 64)]

    def owcopy(n, ref, dev):
        return remote(ref, ref, ow_s, ow_r.at[n], dev)

    ow_out = [
        owcopy(0, head_ref(tp), right_x),
        owcopy(1, head_ref(tp), left_x),
        owcopy(4, head_ref(tp), partner),
        owcopy(2, head_ref(tl, 0), right_x),
        owcopy(3, head_ref(tr, 1), left_x),
        owcopy(4, head_ref(tl), partner),
        owcopy(4, head_ref(tr), partner),
        owcopy(4, head_ref(far, 0), partner),
        owcopy(4, head_ref(far, 1), partner),
    ]
    ow_in = [
        owcopy(0, head_ref(tl), right_x),
        owcopy(1, head_ref(tr), left_x),
        owcopy(2, head_ref(far, 0), right_x),
        owcopy(3, head_ref(far, 1), left_x),
    ]
    loads[6].wait()

    for n in range(3):
        ow_out[n].start()

    def kvb(h, d, k, q):
        shift = (k - 1) * (-1 if d == 0 else 1)
        buf = kv0 if h == 0 else kv1
        ref = buf.at[wrap(pos[h] + shift), q // 2, pl.ds(4 * (q % 2), 4)]
        dev = {axis[h]: wrap(pos[h] + (1 if d == 0 else -1))}
        return remote(ref, ref, kb_s.at[h], kb_r.at[k - 1, q], dev)

    def kv_pass(k):
        if k == 2:
            arrived(kv0.at[0:4], kb_r.at[0, 0])
        for q in range(4):
            if k > 2:
                arrived(kv0.at[0, 0 : 2 if k < 5 else 1], kb_r.at[k - 2, q])
            if k <= 4:
                for h in range(2):
                    for d in range(2):
                        if k < 4 or d == q // 2:
                            kvb(h, d, k, q).start()

    def rest(buf, h, d, k, m, shift):
        lo, hi = (1, RING) if k < 4 else ((1, 5) if d == 0 else (5, RING))
        return buf.at[h, m, wrap(pos[h] + shift * (-1 if d == 0 else 1)), lo:hi]

    def pump_near(m):
        for h in range(2):
            for d in range(2):
                dev = {axis[h]: wrap(pos[h] + (1 if d == 0 else -1))}
                for lo in (1, 6):
                    ref = w.at[h, m, pos[h], lo : lo + 2]
                    remote(ref, ref, wb_s, wb_r.at[0, m], dev).start()

    def pump(k, m):
        if k > 1:
            arrived(w.at[0, m, 0 : 4 if k < 5 else 2, 1:RING], wb_r.at[k - 2, m])
        for h in range(2):
            for d in range(2):
                if k <= 4:
                    ref = rest(w, h, d, k, m, k - 1) if k > 1 else w.at[h, m, pos[h], 3:6]
                    dev = {axis[h]: wrap(pos[h] + (1 if d == 0 else -1))}
                    remote(ref, ref, wb_s, wb_r.at[k - 1, m], dev).start()
        for h in range(2):
            for d in range(2):
                if k > 1:
                    src, dst = rest(w, h, d, k - 1, m, k - 1), rest(wp, h, d, k - 1, m, k - 1)
                    remote(src, dst, wr_s, wr_r.at[m], partner).start()
                elif d == 0:
                    src, dst = rest(w, h, d, 1, m, 0), rest(wp, h, d, 1, m, 0)
                    remote(src, dst, wr_s, wr_r.at[m], partner).start()

    ones = jnp.ones((1, HEAD), BF16)

    def attend(blocks):
        keys = jnp.concatenate([buf[b, 0].reshape(256, HEAD) for buf, b in blocks], axis=0)
        vals = jnp.concatenate([buf[b, 1].reshape(256, HEAD) for buf, b in blocks], axis=0)
        wide = keys.shape[0]
        vals = jnp.concatenate([vals, jnp.broadcast_to(ones, vals.shape)], axis=1)

        def scores_of(h):
            return lax.dot_general(qbuf[h], keys, NT, preferred_element_type=F32)

        scores = scores_of(0)
        for h in range(TEAM):
            later = scores_of(h + 1) if h + 1 < TEAM else None
            old = peak[h]
            new = jnp.maximum(old, jnp.max(scores, axis=1, keepdims=True))
            factor = jnp.exp2(old - new)
            peak[h] = new
            raw = jnp.exp2(scores - jnp.concatenate([new] * (wide // HEAD), axis=1)).astype(BF16)
            update = jnp.dot(raw, vals, preferred_element_type=F32)
            acc[h] = acc[h] * jnp.concatenate([factor, factor], axis=1) + update
            scores = later

    w_first(2)
    kv_group(1)
    kv_group(2)
    kv_group(3)
    kv_group(4)
    w_first(3)
    own_pass(2)
    arrived(qbuf.at[0:3], q_r)
    attend([(kv0, z), (kv1, y)])
    kv_pass(2)
    w_first(4)
    pump_near(0)
    own_pass(3)
    attend([(kv0, wrap(z - 1)), (kv0, wrap(z + 1)), (kv1, wrap(y - 1)), (kv1, wrap(y + 1))])
    kv_pass(3)
    pump_near(1)
    w_first(5)
    pump(1, 0)
    pump(1, 1)
    ow_in[0].wait_recv()
    ow_out[3].start()
    ow_in[1].wait_recv()
    ow_out[4].start()
    ow_out[5].start()
    ow_out[6].start()
    attend([(kv0, wrap(z - 2)), (kv0, wrap(z + 2)), (kv1, wrap(y - 2)), (kv1, wrap(y + 2))])
    kv_pass(4)
    own_pass(4)
    pump_near(2)
    pump(1, 2)
    attend([(kv0, wrap(z - 3)), (kv0, wrap(z + 3)), (kv1, wrap(y - 3)), (kv1, wrap(y + 3))])
    pump(2, 0)
    kv_pass(5)
    pump(2, 1)
    attend([(kv0, wrap(z + 4)), (kv1, wrap(y + 4))])
    own_pass(5)

    lane = lax.broadcasted_iota(jnp.int32, (TOK, HEAD), 1)
    tops = jnp.zeros((TOK, HEAD), F32)
    sums = jnp.ones((TOK, HEAD), F32)
    for h in range(TEAM):
        total = acc[h, :, HEAD:]
        mean = (acc[h, :, :HEAD] / total).astype(BF16)
        osend[:, :, h * HEAD : (h + 1) * HEAD] = mean.reshape(8, ROWS, HEAD)
        tops = jnp.where(lane == h, peak[h], tops)
        sums = jnp.where(lane == h, total, sums)
    level = tops + jnp.log2(sums)
    first = level.astype(BF16).astype(F32)
    second = (level - first).astype(BF16).astype(F32)
    third = level - first - second
    stats = first + pltpu.roll(second, 4, 1) + pltpu.roll(third, 8, 1)
    osend[:, :, TEAM * HEAD :] = stats.astype(BF16).reshape(8, ROWS, HEAD)

    def ocopy(d):
        i = wrap(tp + d)
        return remote(osend.at[i], orecv.at[tp], o_s, o_r, tp_id(i))

    for d in (4, 3, 5, 2, 6, 1, 7):
        ocopy(d).start()
    orecv[tp] = osend[tp]

    pump(2, 2)
    ow_in[2].wait_recv()
    ow_out[7].start()
    ow_in[3].wait_recv()
    ow_out[8].start()
    pump(3, 0)
    pump(3, 1)

    arrived(orecv.at[0:7], o_r)
    for t in range(2):
        levels = []
        for i in range(t * TEAM, (t + 1) * TEAM):
            st = orecv[i, :, TEAM * HEAD :].astype(F32)
            levels.append(st + pltpu.roll(st, HEAD - 4, 1) + pltpu.roll(st, HEAD - 8, 1))
        top = jnp.maximum(jnp.maximum(levels[0], levels[1]), jnp.maximum(levels[2], levels[3]))
        shares = [jnp.exp2(v - top) for v in levels]
        total = shares[0] + shares[1] + shares[2] + shares[3]
        shares = [v / total for v in shares]
        for h in range(TEAM):
            mixed = jnp.zeros((ROWS, HEAD), F32)
            for i in range(TEAM):
                block = orecv[t * TEAM + i, :, h * HEAD : (h + 1) * HEAD].astype(F32)
                mixed = mixed + block * shares[i][:, h : h + 1]
            at = (t * TEAM + h) * HEAD
            att[:, at : at + HEAD] = mixed.astype(BF16)

    arrived(ow.at[0:4], ow_r.at[4])
    loads[7].wait()
    loads[8].wait()
    projected = jnp.dot(att[...], ow[...].reshape(8 * HEAD, D), preferred_element_type=F32)
    middle = (res_ref[...].astype(F32) + projected).astype(BF16)
    mid[...] = middle
    nbuf[x] = normalize(middle.astype(F32), ng_ref[...]).astype(BF16)

    xl, xr, xf = wrap(x - 1, NX), wrap(x + 1, NX), wrap(x + 2, NX)
    low, high = pl.ds(0, 16), pl.ds(16, 16)
    halves = (pl.ds(0, D // 2), pl.ds(D // 2, D // 2))

    def ncopy(n, ref, dev):
        return remote(ref, ref, n_s, n_r.at[n], dev)

    def n_far(d, p):
        if d == 0:
            return ncopy(p, nbuf.at[x, low, halves[p]], right_x)
        return ncopy(2 + p, nbuf.at[x, high, halves[p]], left_x)

    def n_far_on(d, p):
        if d == 0:
            ncopy(p, nbuf.at[xl, low, halves[p]], right_x).wait_recv()
            ncopy(4, nbuf.at[xl, low, halves[p]], right_x).start()
        else:
            ncopy(2 + p, nbuf.at[xr, high, halves[p]], left_x).wait_recv()
            ncopy(4, nbuf.at[xr, high, halves[p]], left_x).start()

    for p in range(2):
        n_far(0, p).start()
        n_far(1, p).start()
    ncopy(4, nbuf.at[x, high], right_x).start()
    ncopy(4, nbuf.at[x, low], left_x).start()
    pump(3, 2)
    pump(4, 0)
    n_far_on(0, 0)
    n_far_on(1, 0)
    pump(4, 1)
    n_far_on(0, 1)
    n_far_on(1, 1)
    pump(4, 2)
    pump(5, 0)
    pump(5, 1)
    arrived(nbuf.at[0:2], n_r.at[4])
    normed = nbuf[...].reshape(NX * ROWS, D)

    def all_of(m):
        return remote(w.at[:, m, :, 1:RING], wp.at[:, m, :, 1:RING], wr_s, wr_r.at[m], partner)

    back_y = [wrap(i - y) for i in range(RING)]
    back_z = [wrap(i - z) for i in range(RING)]

    def matrix(buf, m, places=range(NZ)):
        blocks = []
        for i in places:
            for k in range(NY):
                blocks += [buf[0, m, i, back_y[k]], buf[1, m, k, back_z[i]]]
        return jnp.concatenate(blocks, axis=0)

    def hidden_of(buf):
        gate_part = jnp.dot(normed, matrix(buf, 0), preferred_element_type=F32)
        lifted = jnp.dot(normed, matrix(buf, 1), preferred_element_type=F32)
        return (gate_part / (1.0 + jnp.exp(-gate_part)) * lifted).astype(BF16)

    hidden = hidden_of(w)
    arrived(w.at[:, :, :, 0], wro_r)
    all_of(0).wait_recv()
    all_of(1).wait_recv()
    hidden_p = hidden_of(wp)
    pump(5, 2)
    def pcopy(n, src, dst, dev):
        return remote(src, dst, p_s, p_r.at[n], dev)

    def parts_of(left, buf, cut):
        places = range(4 * cut, 4 * cut + 4)
        parts = lax.dot_general(left, matrix(buf, 2, places), NT, preferred_element_type=F32)
        return parts.reshape(NX, ROWS, D // 2)

    def far_copy(cut, d):
        if d == 0:
            return pcopy(2 * cut, psend.at[cut, xf, low], pfar.at[cut, 0], right_x)
        return pcopy(2 * cut + 1, psend.at[cut, xf, high], pfar.at[cut, 1], left_x)

    def near_copies(cut):
        return [
            pcopy(4, psend.at[cut, xr, high], precv.at[cut, 0, high], right_x),
            pcopy(4, psend.at[cut, xl, low], precv.at[cut, 1, low], left_x),
        ]

    def mix(cut):
        far_copy(cut, 0).wait_recv()
        pmix[cut, 0] = (pown[cut, xr, low] + pfar[cut, 0].astype(F32)).astype(BF16)
        pcopy(4, pmix.at[cut, 0], precv.at[cut, 0, low], right_x).start()
        far_copy(cut, 1).wait_recv()
        pmix[cut, 1] = (pown[cut, xl, high] + pfar[cut, 1].astype(F32)).astype(BF16)
        pcopy(4, pmix.at[cut, 1], precv.at[cut, 1, high], left_x).start()

    for cut in range(2):
        pown[cut] = parts_of(hidden, w, cut)
    all_of(2).wait_recv()
    for cut in range(2):
        parts = pown[cut] + parts_of(hidden_p, wp, cut)
        pown[cut] = parts
        psend[cut] = parts.astype(BF16)
        far_copy(cut, 0).start()
        far_copy(cut, 1).start()
    for cut in range(2):
        for copy in near_copies(cut):
            copy.start()
    mix(0)
    mix(1)

    def drain():
        for h in range(2):
            sent(kv0.at[0, :, 0:7], ka_s.at[h])
            sent(kv0.at[0:7], kb_s.at[h])
        sent(w.at[:, :, 0:7, 0], wa_s)
        sent(w.at[:, :, 0:7, 0], wo_s)
        sent(qbuf.at[0:3], q_s)
        sent(osend.at[0:7], o_s)
        sent(ow.at[0:7], ow_s)
        sent(nbuf.at[0:3], n_s)
        sent(w.at[:, :, 0:7, 1:RING], wb_s)
        sent(w, wr_s)

    def finish():
        for cut in range(2):
            columns = slice(cut * D // 2, (cut + 1) * D // 2)
            total = mid[:, columns].astype(F32) + pown[cut, x]
            total = total + precv[cut, 0].astype(F32) + precv[cut, 1].astype(F32)
            out_ref[:, columns] = total.astype(BF16)
        sent(psend.at[:, 0:3], p_s)

    drain()
    arrived(precv, p_r.at[4])
    finish()


def local(
    queries, keys, values, query_gain, key_gain, residual_in, out_weight, norm_gain,
    gate_weight, up_weight, down_weight,
):
    vmem = pl.BlockSpec(memory_space=pltpu.VMEM)
    dma = pltpu.SemaphoreType.DMA
    tables = [jnp.asarray(t) for t in rope_tables()]
    return pl.pallas_call(
        layer_kernel,
        name="layer",
        out_shape=jax.ShapeDtypeStruct((ROWS, D), BF16),
        in_specs=[pl.BlockSpec(memory_space=pl.ANY)] * 13,
        out_specs=vmem,
        scratch_shapes=[
            pltpu.VMEM((TOK, HEAD), BF16),
            pltpu.VMEM((KTOK, HEAD), BF16),
            pltpu.VMEM((1, HEAD), F32),
            pltpu.VMEM((1, HEAD), F32),
            pltpu.VMEM((ROWS, D), BF16),
            pltpu.VMEM((1, D), F32),
            pltpu.VMEM((2, 4, HEAD), F32),
            pltpu.VMEM((2, GRID_WIDTH, HEAD), F32),
            pltpu.VMEM((TEAM, TOK, HEAD), BF16),
            pltpu.VMEM((NZ, 2, NY, KH, HEAD), BF16),
            pltpu.VMEM((NY, 2, NZ, KH, HEAD), BF16),
            pltpu.VMEM((2, 3, RING, RING, 16, FFD), BF16),
            pltpu.VMEM((2, 3, RING, RING, 16, FFD), BF16),
            pltpu.VMEM((8, HEAD, D), BF16),
            pltpu.VMEM((TEAM, TOK, 2 * HEAD), F32),
            pltpu.VMEM((TEAM, TOK, HEAD), F32),
            pltpu.VMEM((8, ROWS, (TEAM + 1) * HEAD), BF16),
            pltpu.VMEM((8, ROWS, (TEAM + 1) * HEAD), BF16),
            pltpu.VMEM((ROWS, 8 * HEAD), BF16),
            pltpu.VMEM((NX, ROWS, D), BF16),
            pltpu.VMEM((ROWS, D), BF16),
            pltpu.VMEM((2, NX, ROWS, D // 2), BF16),
            pltpu.VMEM((2, NX, ROWS, D // 2), F32),
            pltpu.VMEM((2, 2, ROWS, D // 2), BF16),
            pltpu.VMEM((2, 2, 16, D // 2), BF16),
            pltpu.VMEM((2, 2, 16, D // 2), BF16),
            dma((11,)), dma, dma,
            dma((2,)), dma((4,)),
            dma, dma((4,)),
            dma, dma((4,)),
            dma((2,)), dma((4, 4)),
            dma, dma((4, 3)),
            dma, dma((3,)), dma,
            dma, dma((5,)),
            dma, dma,
            dma, dma((5,)),
            dma, dma((5,)),
        ],
        compiler_params=pltpu.CompilerParams(
            collective_id=0, has_side_effects=True, vmem_limit_bytes=56 * 1024 * 1024
        ),
    )(
        queries, keys, values, query_gain.reshape(1, -1), key_gain.reshape(1, -1), residual_in,
        out_weight, norm_gain.reshape(1, -1),
        *[a.reshape(2, 16, FFD) for a in (gate_weight, up_weight, down_weight.T)], *tables,
    )


def solution(mesh):
    finer = Mesh(mesh.devices.reshape(NZ, NY, NX, 2), ("z", "y", "x", "c"))
    sp, tp = ("z", "y"), ("x", "c")
    in_specs = (
        P(sp, tp),
        P(sp, None),
        P(sp, None),
        P(),
        P(),
        P(sp + tp, None),
        P(tp, None),
        P(),
        P(sp, tp),
        P(sp, tp),
        P(tp, sp),
    )
    return jax.shard_map(
        local, mesh=finer, in_specs=in_specs, out_specs=P(sp + tp, None), check_vma=False
    )
```

```python
import math

import jax
import jax.numpy as jnp
import numpy as np
from jax import lax
from jax.experimental import pallas as pl
from jax.experimental.pallas import tpu as pltpu
from jax.sharding import Mesh
from jax.sharding import PartitionSpec as P

NZ = 8
NY = 8
RING = 8
NX = 4
HEAD = 128
GRID_WIDTH = 64
TOK = 256
TEAM = 4
KTOK = TOK // TEAM
KH = KTOK // 2
ROWS = 32
D = 2048
FFD = 384
EPS = 1e-06
ROPE_BASE = 10000.0
SCALE = HEAD ** (-0.5) * math.log2(math.e)
F32 = jnp.float32
BF16 = jnp.bfloat16
NT = (((1,), (1,)), ((), ()))
FAR_FIRST = (1, 7, 2, 6, 4, 3, 5)


def rope_tables():
    quarter = HEAD // 4
    inverse = ROPE_BASE ** (-np.arange(quarter, dtype=np.float64) * 2.0 / (HEAD // 2))
    rows = np.arange(NZ * NY * TOK // GRID_WIDTH, dtype=np.float64)[:, None] * inverse
    cols = np.arange(GRID_WIDTH, dtype=np.float64)[:, None] * inverse

    def half(angles):
        return (
            np.concatenate([np.cos(angles), np.cos(angles)], axis=1),
            np.concatenate([-np.sin(angles), np.sin(angles)], axis=1),
        )

    rc, rs = half(rows)
    cc, cs = half(cols)
    rc, rs = rc.reshape(-1, 4, HEAD // 2), rs.reshape(-1, 4, HEAD // 2)
    left = lambda a: np.concatenate([a, np.zeros_like(a)], axis=-1).astype(np.float32)
    right = lambda a: np.concatenate([np.zeros_like(a), a], axis=-1).astype(np.float32)
    return np.stack([left(rc), left(rs)], axis=1), np.stack([right(cc), right(cs)])


def normalize(x, gain):
    return x * lax.rsqrt(jnp.mean(x * x, axis=-1, keepdims=True) + EPS) * gain


def turn(x, cosine, sine):
    lane = lax.broadcasted_iota(jnp.int32, x.shape, 1)
    ahead = pltpu.roll(x, HEAD - 32, 1)
    behind = pltpu.roll(x, 32, 1)
    partner = jnp.where((lane // 32) % 2 == 0, ahead, behind)
    return x * cosine + partner * sine


def layer_kernel(
    q_hbm, k_hbm, v_hbm, qg_hbm, kg_hbm, res_hbm, ow_hbm, ng_hbm, gate_hbm, up_hbm, down_hbm,
    row_hbm, col_hbm,
    out_ref,
    q_ref, k_ref, qg_ref, kg_ref, res_ref, ng_ref, row_ref, col_ref,
    qbuf, kv0, kv1, w, wp, ow, acc, peak, osend, orecv, att, nbuf, mid, psend, pown, precv, pfar, pmix,
    in_s, q_s, q_r, ka_s, ka_r, wa_s, wa_r, wo_s, wo_r, kb_s, kb_r, wb_s, wb_r, wr_s, wr_r, wro_r,
    ow_s, ow_r, o_s, o_r, n_s, n_r, p_s, p_r,
):
    z = lax.axis_index("z")
    y = lax.axis_index("y")
    x = lax.axis_index("x")
    c = lax.axis_index("c")
    tp = x * 2 + c
    team = x // 2
    j = lax.rem(x, 2) * 2 + c
    s = z * NY + y
    pos = (z, y)
    axis = ("z", "y")

    def wrap(v, n=RING):
        return lax.rem(v + n, n)

    def tp_id(i):
        return {"x": i // 2, "c": lax.rem(i, 2)}

    barrier = pltpu.get_barrier_semaphore()

    def greet(d, carry):
        pl.semaphore_signal(barrier, inc=1, device_id={"z": wrap(z + d)})
        pl.semaphore_signal(barrier, inc=1, device_id={"y": wrap(y + d)})
        pl.semaphore_signal(barrier, inc=1, device_id=tp_id(wrap(tp + d)))
        return carry

    lax.fori_loop(1, RING, greet, 0)

    lanes = pl.ds(pl.multiple_of(team * HEAD, HEAD), HEAD)

    def key_rows(half):
        return pl.ds(pl.multiple_of(j * KTOK + half * KH, KH), KH)

    loads = [
        (k_hbm.at[pl.ds(pl.multiple_of(j * KTOK, KTOK), KTOK), lanes], k_ref),
        (row_hbm.at[s], row_ref),
        (col_hbm, col_ref),
        (kg_hbm, kg_ref),
        (q_hbm, q_ref),
        (qg_hbm, qg_ref),
        (ow_hbm, ow.at[tp]),
        (res_hbm, res_ref),
        (ng_hbm, ng_ref),
        (v_hbm.at[key_rows(0), lanes], kv0.at[z, 1, y]),
        (v_hbm.at[key_rows(1), lanes], kv1.at[y, 1, z]),
        (gate_hbm.at[0], w.at[0, 0, z, 0]),
        (gate_hbm.at[1], w.at[1, 0, y, 0]),
        (up_hbm.at[0], w.at[0, 1, z, 0]),
        (up_hbm.at[1], w.at[1, 1, y, 0]),
        (down_hbm.at[0], w.at[0, 2, z, 0]),
        (down_hbm.at[1], w.at[1, 2, y, 0]),
    ]
    sems = [in_s.at[n] for n in (0, 1, 2, 3, 4, 5, 6, 7, 8, 9, 9, 10, 10, 10, 10, 10, 10)]
    loads = [pltpu.make_async_copy(a, b, m) for (a, b), m in zip(loads, sems)]

    def landed(ref, sem):
        pltpu.make_async_copy(ref, ref, sem).wait()

    for load in loads:
        load.start()

    for load in loads[:4]:
        load.wait()
    cosine = row_ref[0, pl.ds(j, 1), :] + col_ref[0]
    sine = row_ref[1, pl.ds(j, 1), :] + col_ref[1]
    kk = k_ref[...].astype(F32)
    kk = turn(normalize(kk, kg_ref[...]), cosine, sine).astype(BF16)
    kv0[z, 0, y] = kk[:KH]
    kv1[y, 0, z] = kk[KH:]
    landed(kv0.at[z, 1, 0:2], in_s.at[9])
    pl.semaphore_wait(barrier, 21)

    partner = {"c": 1 - c}

    def remote(ref, dst, ss, rs, dev):
        return pltpu.make_async_remote_copy(
            src_ref=ref, dst_ref=dst, send_sem=ss, recv_sem=rs,
            device_id=dev, device_id_type=pl.DeviceIdType.MESH,
        )

    def arrived(ref, sem):
        remote(ref, ref, sem, sem, partner).wait_recv()

    def sent(ref, sem):
        remote(ref, ref, sem, sem, partner).wait_send()

    def kva(h, d):
        ref = kv0.at[z, :, y] if h == 0 else kv1.at[y, :, z]
        dev = {"y": wrap(y + d)} if h == 0 else {"z": wrap(z + d)}
        return remote(ref, ref, ka_s.at[h], ka_r.at[min(d, RING - d) - 1], dev)

    def wa(h, d, k):
        src, dst = ((1 - k) % RING, -k % RING) if d == 0 else (k - 1, k)
        pick = slice(0, 3) if k < 4 else (slice(0, 2) if d == 0 else slice(2, 3))
        step = 1 if d == 0 else -1
        dev = {"y": wrap(y + step)} if h == 0 else {"z": wrap(z + step)}
        return remote(
            w.at[h, pick, pos[h], src], w.at[h, pick, pos[h], dst], wa_s, wa_r.at[k - 1], dev
        )

    def four(k):
        return w.at[0, :, 0 : 4 if k < 5 else 2, 0]

    def w_first(k):
        if k > 1:
            arrived(four(k), wa_r.at[k - 2])
        if k <= 4:
            for h in range(2):
                for d in range(2):
                    wa(h, d, k).start()

    def own_ref(buf, h, d, k, shift):
        pick = slice(0, 3) if k < 4 else (slice(0, 2) if d == 0 else slice(2, 3))
        return buf.at[h, pick, wrap(pos[h] + shift * (-1 if d == 0 else 1)), 0]

    def own_pass(k):
        if k > 1:
            arrived(four(k), wo_r.at[k - 2])
        for h in range(2):
            for d in range(2):
                if k <= 4:
                    ref = own_ref(w, h, d, k, k - 1)
                    dev = {axis[h]: wrap(pos[h] + (1 if d == 0 else -1))}
                    remote(ref, ref, wo_s, wo_r.at[k - 1], dev).start()
        for h in range(2):
            for d in range(2):
                if k > 1:
                    src, dst = own_ref(w, h, d, k - 1, k - 1), own_ref(wp, h, d, k - 1, k - 1)
                    remote(src, dst, wr_s, wro_r, partner).start()
                elif d == 0:
                    src, dst = own_ref(w, h, d, 1, 0), own_ref(wp, h, d, 1, 0)
                    remote(src, dst, wr_s, wro_r, partner).start()

    def kv_piece(h, e):
        ref = kv0.at[z, :, wrap(y + e)] if h == 0 else kv1.at[y, :, wrap(z + e)]
        for d in range(2):
            dev = {axis[h]: wrap(pos[h] + (1 if d == 0 else -1))}
            remote(ref, ref, kb_s.at[h], kb_r.at[0, 0], dev).start()

    def kv_group(g):
        if g > 0:
            arrived(kv0.at[0, :, 0 : 4 if g < 4 else 2], ka_r.at[g - 1])
        for h in range(2):
            for e in sorted({g % RING, -g % RING}):
                kv_piece(h, e)

    def start_kva(d):
        kva(0, d).start()
        kva(1, d).start()

    kv_group(0)
    landed(w.at[:, :, 0, 0], in_s.at[10])
    w_first(1)
    for d in FAR_FIRST:
        start_kva(d)
    own_pass(1)

    loads[4].wait()
    loads[5].wait()
    for r in range(4):
        part = slice(r * GRID_WIDTH, (r + 1) * GRID_WIDTH)
        cosine = row_ref[0, r : r + 1, :] + col_ref[0]
        sine = row_ref[1, r : r + 1, :] + col_ref[1]
        qq = turn(normalize(q_ref[part, :].astype(F32), qg_ref[...]), cosine, sine)
        qbuf[j, part] = (qq * SCALE).astype(BF16)
    peak[...] = jnp.full(peak.shape, -1e30, F32)
    acc[...] = jnp.zeros(acc.shape, F32)

    def qcopy(d):
        other = team * TEAM + lax.rem(j + d, TEAM)
        return remote(qbuf.at[j], qbuf.at[j], q_s, q_r, tp_id(other))

    for d in range(1, TEAM):
        qcopy(d).start()

    right_x = {"x": wrap(x + 1, NX)}
    left_x = {"x": wrap(x - 1, NX)}
    tl = wrap(x - 1, NX) * 2 + c
    tr = wrap(x + 1, NX) * 2 + c
    far = wrap(x + 2, NX) * 2 + c

    def head_ref(i, part=None):
        if part is None:
            return ow.at[i]
        return ow.at[i, pl.ds(part * 64, 64)]

    def owcopy(n, ref, dev):
        return remote(ref, ref, ow_s, ow_r.at[n], dev)

    ow_out = [
        owcopy(0, head_ref(tp), right_x),
        owcopy(1, head_ref(tp), left_x),
        owcopy(4, head_ref(tp), partner),
        owcopy(2, head_ref(tl, 0), right_x),
        owcopy(3, head_ref(tr, 1), left_x),
        owcopy(4, head_ref(tl), partner),
        owcopy(4, head_ref(tr), partner),
        owcopy(4, head_ref(far, 0), partner),
        owcopy(4, head_ref(far, 1), partner),
    ]
    ow_in = [
        owcopy(0, head_ref(tl), right_x),
        owcopy(1, head_ref(tr), left_x),
        owcopy(2, head_ref(far, 0), right_x),
        owcopy(3, head_ref(far, 1), left_x),
    ]
    loads[6].wait()

    for n in range(3):
        ow_out[n].start()

    def kvb(h, d, k, q):
        shift = (k - 1) * (-1 if d == 0 else 1)
        buf = kv0 if h == 0 else kv1
        ref = buf.at[wrap(pos[h] + shift), q // 2, pl.ds(4 * (q % 2), 4)]
        dev = {axis[h]: wrap(pos[h] + (1 if d == 0 else -1))}
        return remote(ref, ref, kb_s.at[h], kb_r.at[k - 1, q], dev)

    def kv_pass(k):
        if k == 2:
            arrived(kv0.at[0:4], kb_r.at[0, 0])
        for q in range(4):
            if k > 2:
                arrived(kv0.at[0, 0 : 2 if k < 5 else 1], kb_r.at[k - 2, q])
            if k <= 4:
                for h in range(2):
                    for d in range(2):
                        if k < 4 or d == q // 2:
                            kvb(h, d, k, q).start()

    def rest(buf, h, d, k, m, shift):
        lo, hi = (1, RING) if k < 4 else ((1, 5) if d == 0 else (5, RING))
        return buf.at[h, m, wrap(pos[h] + shift * (-1 if d == 0 else 1)), lo:hi]

    def pump_near(m):
        for h in range(2):
            for d in range(2):
                dev = {axis[h]: wrap(pos[h] + (1 if d == 0 else -1))}
                for lo in (1, 6):
                    ref = w.at[h, m, pos[h], lo : lo + 2]
                    remote(ref, ref, wb_s, wb_r.at[0, m], dev).start()

    def pump(k, m):
        if k > 1:
            arrived(w.at[0, m, 0 : 4 if k < 5 else 2, 1:RING], wb_r.at[k - 2, m])
        for h in range(2):
            for d in range(2):
                if k <= 4:
                    ref = rest(w, h, d, k, m, k - 1) if k > 1 else w.at[h, m, pos[h], 3:6]
                    dev = {axis[h]: wrap(pos[h] + (1 if d == 0 else -1))}
                    remote(ref, ref, wb_s, wb_r.at[k - 1, m], dev).start()
        for h in range(2):
            for d in range(2):
                if k > 1:
                    src, dst = rest(w, h, d, k - 1, m, k - 1), rest(wp, h, d, k - 1, m, k - 1)
                    remote(src, dst, wr_s, wr_r.at[m], partner).start()
                elif d == 0:
                    src, dst = rest(w, h, d, 1, m, 0), rest(wp, h, d, 1, m, 0)
                    remote(src, dst, wr_s, wr_r.at[m], partner).start()

    ones = jnp.ones((1, HEAD), BF16)

    def attend(blocks):
        keys = jnp.concatenate([buf[b, 0].reshape(256, HEAD) for buf, b in blocks], axis=0)
        vals = jnp.concatenate([buf[b, 1].reshape(256, HEAD) for buf, b in blocks], axis=0)
        wide = keys.shape[0]
        vals = jnp.concatenate([vals, jnp.broadcast_to(ones, vals.shape)], axis=1)

        def scores_of(h):
            return lax.dot_general(qbuf[h], keys, NT, preferred_element_type=F32)

        scores = scores_of(0)
        for h in range(TEAM):
            later = scores_of(h + 1) if h + 1 < TEAM else None
            old = peak[h]
            new = jnp.maximum(old, jnp.max(scores, axis=1, keepdims=True))
            factor = jnp.exp2(old - new)
            peak[h] = new
            raw = jnp.exp2(scores - jnp.concatenate([new] * (wide // HEAD), axis=1)).astype(BF16)
            update = jnp.dot(raw, vals, preferred_element_type=F32)
            acc[h] = acc[h] * jnp.concatenate([factor, factor], axis=1) + update
            scores = later

    w_first(2)
    kv_group(1)
    kv_group(2)
    kv_group(3)
    kv_group(4)
    w_first(3)
    own_pass(2)
    arrived(qbuf.at[0:3], q_r)
    attend([(kv0, z), (kv1, y)])
    kv_pass(2)
    w_first(4)
    pump_near(0)
    own_pass(3)
    attend([(kv0, wrap(z - 1)), (kv0, wrap(z + 1)), (kv1, wrap(y - 1)), (kv1, wrap(y + 1))])
    kv_pass(3)
    pump_near(1)
    w_first(5)
    pump(1, 0)
    pump(1, 1)
    ow_in[0].wait_recv()
    ow_out[3].start()
    ow_in[1].wait_recv()
    ow_out[4].start()
    ow_out[5].start()
    ow_out[6].start()
    attend([(kv0, wrap(z - 2)), (kv0, wrap(z + 2)), (kv1, wrap(y - 2)), (kv1, wrap(y + 2))])
    kv_pass(4)
    own_pass(4)
    pump_near(2)
    pump(1, 2)
    attend([(kv0, wrap(z - 3)), (kv0, wrap(z + 3)), (kv1, wrap(y - 3)), (kv1, wrap(y + 3))])
    pump(2, 0)
    kv_pass(5)
    pump(2, 1)
    attend([(kv0, wrap(z + 4)), (kv1, wrap(y + 4))])
    own_pass(5)

    lane = lax.broadcasted_iota(jnp.int32, (TOK, HEAD), 1)
    tops = jnp.zeros((TOK, HEAD), F32)
    sums = jnp.ones((TOK, HEAD), F32)
    for h in range(TEAM):
        total = acc[h, :, HEAD:]
        mean = (acc[h, :, :HEAD] / total).astype(BF16)
        osend[:, :, h * HEAD : (h + 1) * HEAD] = mean.reshape(8, ROWS, HEAD)
        tops = jnp.where(lane == h, peak[h], tops)
        sums = jnp.where(lane == h, total, sums)
    level = tops + jnp.log2(sums)
    first = level.astype(BF16).astype(F32)
    second = (level - first).astype(BF16).astype(F32)
    third = level - first - second
    stats = first + pltpu.roll(second, 4, 1) + pltpu.roll(third, 8, 1)
    osend[:, :, TEAM * HEAD :] = stats.astype(BF16).reshape(8, ROWS, HEAD)

    def ocopy(d):
        i = wrap(tp + d)
        return remote(osend.at[i], orecv.at[tp], o_s, o_r, tp_id(i))

    for d in (4, 3, 5, 2, 6, 1, 7):
        ocopy(d).start()
    orecv[tp] = osend[tp]

    pump(2, 2)
    ow_in[2].wait_recv()
    ow_out[7].start()
    ow_in[3].wait_recv()
    ow_out[8].start()
    pump(3, 0)
    pump(3, 1)

    arrived(orecv.at[0:7], o_r)
    for t in range(2):
        levels = []
        for i in range(t * TEAM, (t + 1) * TEAM):
            st = orecv[i, :, TEAM * HEAD :].astype(F32)
            levels.append(st + pltpu.roll(st, HEAD - 4, 1) + pltpu.roll(st, HEAD - 8, 1))
        top = jnp.maximum(jnp.maximum(levels[0], levels[1]), jnp.maximum(levels[2], levels[3]))
        shares = [jnp.exp2(v - top) for v in levels]
        total = shares[0] + shares[1] + shares[2] + shares[3]
        shares = [v / total for v in shares]
        for h in range(TEAM):
            mixed = jnp.zeros((ROWS, HEAD), F32)
            for i in range(TEAM):
                block = orecv[t * TEAM + i, :, h * HEAD : (h + 1) * HEAD].astype(F32)
                mixed = mixed + block * shares[i][:, h : h + 1]
            at = (t * TEAM + h) * HEAD
            att[:, at : at + HEAD] = mixed.astype(BF16)

    arrived(ow.at[0:4], ow_r.at[4])
    loads[7].wait()
    loads[8].wait()
    projected = jnp.dot(att[...], ow[...].reshape(8 * HEAD, D), preferred_element_type=F32)
    middle = (res_ref[...].astype(F32) + projected).astype(BF16)
    mid[...] = middle
    nbuf[x] = normalize(middle.astype(F32), ng_ref[...]).astype(BF16)

    xl, xr, xf = wrap(x - 1, NX), wrap(x + 1, NX), wrap(x + 2, NX)
    low, high = pl.ds(0, 16), pl.ds(16, 16)
    halves = (pl.ds(0, D // 2), pl.ds(D // 2, D // 2))

    def ncopy(n, ref, dev):
        return remote(ref, ref, n_s, n_r.at[n], dev)

    def n_far(d, p):
        if d == 0:
            return ncopy(p, nbuf.at[x, low, halves[p]], right_x)
        return ncopy(2 + p, nbuf.at[x, high, halves[p]], left_x)

    def n_far_on(d, p):
        if d == 0:
            ncopy(p, nbuf.at[xl, low, halves[p]], right_x).wait_recv()
            ncopy(4, nbuf.at[xl, low, halves[p]], right_x).start()
        else:
            ncopy(2 + p, nbuf.at[xr, high, halves[p]], left_x).wait_recv()
            ncopy(4, nbuf.at[xr, high, halves[p]], left_x).start()

    for p in range(2):
        n_far(0, p).start()
        n_far(1, p).start()
    ncopy(4, nbuf.at[x, high], right_x).start()
    ncopy(4, nbuf.at[x, low], left_x).start()
    pump(3, 2)
    pump(4, 0)
    n_far_on(0, 0)
    n_far_on(1, 0)
    pump(4, 1)
    n_far_on(0, 1)
    n_far_on(1, 1)
    pump(4, 2)
    pump(5, 0)
    pump(5, 1)
    arrived(nbuf.at[0:2], n_r.at[4])
    normed = nbuf[...].reshape(NX * ROWS, D)

    def all_of(m):
        return remote(w.at[:, m, :, 1:RING], wp.at[:, m, :, 1:RING], wr_s, wr_r.at[m], partner)

    back_y = [wrap(i - y) for i in range(RING)]
    back_z = [wrap(i - z) for i in range(RING)]

    def matrix(buf, m, places=range(NZ)):
        blocks = []
        for i in places:
            for k in range(NY):
                blocks += [buf[0, m, i, back_y[k]], buf[1, m, k, back_z[i]]]
        return jnp.concatenate(blocks, axis=0)

    def hidden_of(buf):
        gate_part = jnp.dot(normed, matrix(buf, 0), preferred_element_type=F32)
        lifted = jnp.dot(normed, matrix(buf, 1), preferred_element_type=F32)
        return (gate_part / (1.0 + jnp.exp(-gate_part)) * lifted).astype(BF16)

    def pcopy(n, src, dst, dev):
        return remote(src, dst, p_s, p_r.at[n], dev)

    def parts_of(left, buf, cut):
        places = range(4 * cut, 4 * cut + 4)
        parts = lax.dot_general(left, matrix(buf, 2, places), NT, preferred_element_type=F32)
        return parts.reshape(NX, ROWS, D // 2)

    def far_copy(cut, d):
        if d == 0:
            return pcopy(2 * cut, psend.at[cut, xf, low], pfar.at[cut, 0], right_x)
        return pcopy(2 * cut + 1, psend.at[cut, xf, high], pfar.at[cut, 1], left_x)

    def near_copies(cut):
        return [
            pcopy(4, psend.at[cut, xr, high], precv.at[cut, 0, high], right_x),
            pcopy(4, psend.at[cut, xl, low], precv.at[cut, 1, low], left_x),
        ]

    def mix(cut):
        far_copy(cut, 0).wait_recv()
        pmix[cut, 0] = (pown[cut, xr, low] + pfar[cut, 0].astype(F32)).astype(BF16)
        pcopy(4, pmix.at[cut, 0], precv.at[cut, 0, low], right_x).start()
        far_copy(cut, 1).wait_recv()
        pmix[cut, 1] = (pown[cut, xl, high] + pfar[cut, 1].astype(F32)).astype(BF16)
        pcopy(4, pmix.at[cut, 1], precv.at[cut, 1, high], left_x).start()

    hidden = hidden_of(w)
    pump(5, 2)
    for cut in range(2):
        pown[cut] = parts_of(hidden, w, cut)
    arrived(w.at[:, :, :, 0], wro_r)
    all_of(0).wait_recv()
    all_of(1).wait_recv()
    hidden_p = hidden_of(wp)
    all_of(2).wait_recv()
    for cut in range(2):
        parts = pown[cut] + parts_of(hidden_p, wp, cut)
        pown[cut] = parts
        psend[cut] = parts.astype(BF16)
        far_copy(cut, 0).start()
        far_copy(cut, 1).start()
    for cut in range(2):
        for copy in near_copies(cut):
            copy.start()
    mix(0)
    mix(1)

    def drain():
        for h in range(2):
            sent(kv0.at[0, :, 0:7], ka_s.at[h])
            sent(kv0.at[0:7], kb_s.at[h])
        sent(w.at[:, :, 0:7, 0], wa_s)
        sent(w.at[:, :, 0:7, 0], wo_s)
        sent(qbuf.at[0:3], q_s)
        sent(osend.at[0:7], o_s)
        sent(ow.at[0:7], ow_s)
        sent(nbuf.at[0:3], n_s)
        sent(w.at[:, :, 0:7, 1:RING], wb_s)
        sent(w, wr_s)

    def finish():
        for cut in range(2):
            columns = slice(cut * D // 2, (cut + 1) * D // 2)
            total = mid[:, columns].astype(F32) + pown[cut, x]
            total = total + precv[cut, 0].astype(F32) + precv[cut, 1].astype(F32)
            out_ref[:, columns] = total.astype(BF16)
        sent(psend.at[:, 0:3], p_s)

    drain()
    arrived(precv, p_r.at[4])
    finish()


def local(
    queries, keys, values, query_gain, key_gain, residual_in, out_weight, norm_gain,
    gate_weight, up_weight, down_weight,
):
    vmem = pl.BlockSpec(memory_space=pltpu.VMEM)
    dma = pltpu.SemaphoreType.DMA
    tables = [jnp.asarray(t) for t in rope_tables()]
    return pl.pallas_call(
        layer_kernel,
        name="layer",
        out_shape=jax.ShapeDtypeStruct((ROWS, D), BF16),
        in_specs=[pl.BlockSpec(memory_space=pl.ANY)] * 13,
        out_specs=vmem,
        scratch_shapes=[
            pltpu.VMEM((TOK, HEAD), BF16),
            pltpu.VMEM((KTOK, HEAD), BF16),
            pltpu.VMEM((1, HEAD), F32),
            pltpu.VMEM((1, HEAD), F32),
            pltpu.VMEM((ROWS, D), BF16),
            pltpu.VMEM((1, D), F32),
            pltpu.VMEM((2, 4, HEAD), F32),
            pltpu.VMEM((2, GRID_WIDTH, HEAD), F32),
            pltpu.VMEM((TEAM, TOK, HEAD), BF16),
            pltpu.VMEM((NZ, 2, NY, KH, HEAD), BF16),
            pltpu.VMEM((NY, 2, NZ, KH, HEAD), BF16),
            pltpu.VMEM((2, 3, RING, RING, 16, FFD), BF16),
            pltpu.VMEM((2, 3, RING, RING, 16, FFD), BF16),
            pltpu.VMEM((8, HEAD, D), BF16),
            pltpu.VMEM((TEAM, TOK, 2 * HEAD), F32),
            pltpu.VMEM((TEAM, TOK, HEAD), F32),
            pltpu.VMEM((8, ROWS, (TEAM + 1) * HEAD), BF16),
            pltpu.VMEM((8, ROWS, (TEAM + 1) * HEAD), BF16),
            pltpu.VMEM((ROWS, 8 * HEAD), BF16),
            pltpu.VMEM((NX, ROWS, D), BF16),
            pltpu.VMEM((ROWS, D), BF16),
            pltpu.VMEM((2, NX, ROWS, D // 2), BF16),
            pltpu.VMEM((2, NX, ROWS, D // 2), F32),
            pltpu.VMEM((2, 2, ROWS, D // 2), BF16),
            pltpu.VMEM((2, 2, 16, D // 2), BF16),
            pltpu.VMEM((2, 2, 16, D // 2), BF16),
            dma((11,)), dma, dma,
            dma((2,)), dma((4,)),
            dma, dma((4,)),
            dma, dma((4,)),
            dma((2,)), dma((4, 4)),
            dma, dma((4, 3)),
            dma, dma((3,)), dma,
            dma, dma((5,)),
            dma, dma,
            dma, dma((5,)),
            dma, dma((5,)),
        ],
        compiler_params=pltpu.CompilerParams(
            collective_id=0, has_side_effects=True, vmem_limit_bytes=56 * 1024 * 1024
        ),
    )(
        queries, keys, values, query_gain.reshape(1, -1), key_gain.reshape(1, -1), residual_in,
        out_weight, norm_gain.reshape(1, -1),
        *[a.reshape(2, 16, FFD) for a in (gate_weight, up_weight, down_weight.T)], *tables,
    )


def solution(mesh):
    finer = Mesh(mesh.devices.reshape(NZ, NY, NX, 2), ("z", "y", "x", "c"))
    sp, tp = ("z", "y"), ("x", "c")
    in_specs = (
        P(sp, tp),
        P(sp, None),
        P(sp, None),
        P(),
        P(),
        P(sp + tp, None),
        P(tp, None),
        P(),
        P(sp, tp),
        P(sp, tp),
        P(tp, sp),
    )
    return jax.shard_map(
        local, mesh=finer, in_specs=in_specs, out_specs=P(sp + tp, None), check_vma=False
    )
```
